32 devices in a mesh: fs: 8 (over z, y), tp: 4 (over x, core).
Axes of the slice: x: 2, y: 2, z: 4, core: 2. Of those that a mesh axis runs over, the one named last changes fastest.
Arguments:
- fresh_rows: bfloat16 [4096, 2048], P('fs'), may hold values from -6 to 6
- saved_rows: bfloat16 [4096, 2048], P('fs'), may hold values from -6 to 6
- upstream_grad: bfloat16 [4096, 2048], P('fs'), may hold values from -6 to 6
- proj_up: bfloat16 [2048, 8192], P('fs', 'tp'), may hold values from -0.125 to 0.125
- proj_down: bfloat16 [2048, 8192], P('fs', 'tp'), may hold values from -0.0625 to 0.0625
- accum_up: float32 [2048, 8192], P('fs', 'tp'), may hold values from -6 to 6
- accum_down: float32 [2048, 8192], P('fs', 'tp'), may hold values from -6 to 6
Outputs:
- fresh_out: bfloat16 [4096, 2048], P(('fs', 'tp'))
- saved_grad: bfloat16 [4096, 2048], P(('fs', 'tp'))
- accum_up_out: float32 [2048, 8192], P('fs', 'tp')
- accum_down_out: float32 [2048, 8192], P('fs', 'tp')
The draws below stay inside these ranges and needn't reach their ends.
All inputs are finite; a program needn't handle non-finite values.
Results may differ from the reference program's by a relative error of at most 0.014.
Values may be sent and summed in bfloat16 or wider, within the bound.
A program may use at most 128 MiB of HBM per device.

```python
import jax
import jax.numpy as jnp
from jax import lax

D = 2048
FF = 8192
TOKENS = 4096
N_TP = 4


def raised(result, stream_key, source, target, shards_of, factor):
    owner, partner = [(jnp.arange(result.shape[axis_at]) // (result.shape[axis_at] // shards_of)).reshape([-1 if axis == axis_at else 1 for axis in range(result.ndim)]) for axis_at in (source, target)]
    chosen = jax.random.permutation(stream_key, shards_of)[partner]
    strong = (owner == chosen) | (owner == (partner + shards_of // 2) % shards_of)
    return jnp.where(strong, factor * result, result)


def block_levels(key, dims, split, least, top_value):
    factor_of = 1.0
    for axis_at, parts in split:
        draws = jax.random.uniform(jax.random.fold_in(jax.random.fold_in(key, 6), axis_at), (parts,), jnp.float32, least / len(split), top_value / len(split))
        factor_of = factor_of * jnp.repeat(jnp.exp(draws), dims[axis_at] // parts).reshape((-1,) + (1,) * (len(dims) - 1 - axis_at))
    return factor_of


def gaussian(stream_key, extent, spread, reach, shards=(), held_as=jnp.bfloat16):
    level = block_levels(stream_key, extent, shards, -0.22, 0.18) if shards else 1.0
    values = jax.random.normal(stream_key, extent, jnp.float32) * spread * level
    return jnp.minimum(jnp.maximum(values, -reach), reach).astype(held_as)


def heavy_noise(rng, dims, spread, bound, cuts, heavy, held_as=jnp.bfloat16):
    drawn = spread * jax.random.normal(rng, dims, jnp.float32)
    if cuts:
        drawn = drawn * block_levels(rng, dims, cuts, -0.22, 0.18)
    return jnp.clip(raised(drawn, jax.random.fold_in(rng, 3), *heavy), -bound, bound).astype(held_as)


def setup_inputs(seed: int = 0) -> dict:
    splits = jax.random.split(jax.random.key(seed), 8)
    return {
        "fresh_rows": gaussian(splits[0], (TOKENS, D), 1.0, 6.0, ((0, 8),)),
        "saved_rows": gaussian(splits[1], (TOKENS, D), 1.0, 6.0, ((0, 8),)),
        "upstream_grad": heavy_noise(splits[2], (TOKENS, D), 1.0, 6.0, ((0, 8),), (0, 1, 8, 2.0)),
        "proj_up": gaussian(splits[3], (D, FF), D ** -0.5, 0.125, ((0, 8), (1, 4))),
        "proj_down": gaussian(splits[4], (D, FF), FF ** -0.5, 0.0625, ((0, 8), (1, 4))),
        "accum_up": gaussian(splits[5], (D, FF), 1.0, 6.0, ((0, 8), (1, 4)), jnp.float32),
        "accum_down": gaussian(splits[6], (D, FF), 1.0, 6.0, ((0, 8), (1, 4)), jnp.float32),
    }


def block_sum(left, right):
    width = FF // N_TP

    def add_block(index, running):
        first = (index * width).astype(jnp.int32)
        left_part = lax.dynamic_slice_in_dim(left, first, width, 1)
        right_part = lax.dynamic_slice_in_dim(right, first, width, 1)
        partial_sum = jnp.dot(left_part, right_part.T, preferred_element_type=jnp.float32)
        rounded = lax.optimization_barrier(partial_sum.astype(jnp.bfloat16))
        return running + rounded.astype(jnp.float32)

    empty = jnp.zeros((left.shape[0], right.shape[0]), jnp.float32)
    return lax.fori_loop(0, N_TP, add_block, empty).astype(jnp.bfloat16)


def reference(fresh_rows, saved_rows, upstream_grad, proj_up, proj_down, accum_up, accum_down):
    grad_scale = float(TOKENS) ** -0.5
    fresh_pre = jnp.dot(fresh_rows, proj_up, preferred_element_type=jnp.float32)
    fresh_active = jnp.maximum(fresh_pre, 0.0)
    fresh_hidden = (fresh_active * fresh_active).astype(jnp.bfloat16)
    fresh_out = block_sum(fresh_hidden, proj_down)
    saved_pre = jnp.dot(saved_rows, proj_up, preferred_element_type=jnp.float32)
    saved_active = jnp.maximum(saved_pre, 0.0)
    saved_hidden = (saved_active * saved_active).astype(jnp.bfloat16)
    hidden_grad = jnp.dot(upstream_grad, proj_down, preferred_element_type=jnp.float32)
    pre_grad = (2.0 * saved_active * hidden_grad).astype(jnp.bfloat16)
    saved_grad = block_sum(pre_grad, proj_up)
    up_term = jnp.dot(saved_rows.T, pre_grad, preferred_element_type=jnp.float32)
    down_term = jnp.dot(upstream_grad.T, saved_hidden, preferred_element_type=jnp.float32)
    accum_up_out = accum_up + grad_scale * up_term
    accum_down_out = accum_down + grad_scale * down_term
    return fresh_out, saved_grad, accum_up_out, accum_down_out
```

```python
import functools

import jax
import jax.numpy as jnp
from jax import lax
from jax.experimental import pallas as pl
from jax.experimental.pallas import tpu as pltpu
from jax.sharding import PartitionSpec as P


BF = jnp.bfloat16
F32 = jnp.float32


def against_rows(left, right):
    return lax.dot_general(left, right, (((1,), (1,)), ((), ())), preferred_element_type=F32)


def over_tokens(left, right):
    return lax.dot_general(left, right, (((0,), (0,)), ((), ())), preferred_element_type=F32)


def squared_relu(pre_values):
    active = jnp.maximum(pre_values, 0.0)
    return (active, (active * active).astype(BF))


def after(value, *earlier):
    return lax.optimization_barrier((value, earlier))[0]


def body(fresh_rows, saved_rows, upstream_grad, proj_up, proj_down, accum_up, accum_down):
    fs_n, tp_n = lax.axis_size("fs"), lax.axis_size("tp")
    line_n = fs_n // 2
    fs, tp = lax.axis_index("fs"), lax.axis_index("tp")
    line, side = fs // 2, fs % 2
    row_count, width = fresh_rows.shape
    depth, columns = proj_up.shape
    half = columns // 2
    grad_scale = float(row_count * fs_n) ** (-0.5)

    def to_side(value):
        return lax.ppermute(value, "fs", [(i, i ^ 1) for i in range(fs_n)])

    def to_tp(value, bit):
        return lax.ppermute(value, "tp", [(j, j ^ bit) for j in range(tp_n)])

    def along(value, lines, way):
        return lax.ppermute(
            value,
            "fs",
            [(l * 2 + s, (l + way) * 2 + s) for l in lines for s in range(2)],
        )

    def side_block(weight):
        mine = lax.dynamic_slice_in_dim(weight, side * half, half, 1)
        other = lax.dynamic_slice_in_dim(weight, (1 - side) * half, half, 1)
        return mine, to_side(other)

    def line_gather(block, ties={}):
        ups, downs = [block], [block]
        for step in range(1, line_n):
            up, down = after((ups[-1], downs[-1]), *ties.get(step, ()))
            up = along(up, range(step - 1, line_n - 1), 1)
            down = along(down, range(1, line_n - step + 1), -1)
            up, down = lax.optimization_barrier((up, down))
            ups.append(up)
            downs.append(down)
        blocks = [block] + [
            jnp.where(line >= k, ups[k], downs[line_n - k]) for k in range(1, line_n)
        ]
        return jnp.concatenate(blocks, axis=0), ups

    def line_sum(grads, ties={}):
        size = 2 * depth
        up = down = None
        marks = []
        for step in range(1, line_n):
            low = grads[step * size : (step + 1) * size]
            high = grads[(line_n - step) * size : (line_n - step + 1) * size]
            low = low if up is None else low + up.astype(F32)
            high = high if down is None else high + down.astype(F32)
            low, high = after((low.astype(BF), high.astype(BF)), *ties.get(step, ()))
            up = along(low, range(0, step), 1)
            down = along(high, range(line_n - step, line_n), -1)
            up, down = lax.optimization_barrier((up, down))
            marks.append(up)
        return grads[:size] + up.astype(F32) + down.astype(F32), marks

    def finish_grad(accum, total, other):
        mine = total[:depth]
        other = other.astype(F32)
        return accum + jnp.where(
            side == 0,
            jnp.concatenate((mine, other), axis=1),
            jnp.concatenate((other, mine), axis=1),
        )

    order = [lax.rem(line - k + line_n, line_n) * 2 + (side ^ j) for k in range(line_n) for j in range(2)]
    core = tp % 2

    def near_rows(rows):
        piece = row_count // 2
        return to_side(lax.dynamic_slice_in_dim(rows, core * piece, piece, 0))

    def both_sides(rows, near):
        far = to_tp(near, 1)
        rows = jnp.concatenate(
            (rows, jnp.where(core == 0, near, far), jnp.where(core == 0, far, near)), axis=0
        )
        return jnp.concatenate(
            [lax.dynamic_slice_in_dim(rows, o * depth, depth, 1) for o in order], axis=1
        )

    def share_tp(term):
        value = term.astype(BF)
        bit, stages = 1, []
        outer = 2 * tp_n
        rest = row_count // tp_n
        value = value.reshape(2 * tp_n, rest, width)
        while bit < tp_n:
            outer //= 2
            view = value.reshape(outer, 2, rest, width)
            mine = (tp // bit) % 2
            keep = lax.dynamic_index_in_dim(view, mine, 1, keepdims=False)
            send = lax.dynamic_index_in_dim(view, 1 - mine, 1, keepdims=False)
            value = (keep.astype(F32) + to_tp(send, bit).astype(F32)).astype(BF)
            bit *= 2
            stages.append(value)
        return stages

    def share_side(value):
        blocks = [
            lax.dynamic_slice_in_dim(
                value, (lax.rem(line - b // 2 + line_n, line_n) * 2 + (side ^ (b % 2))) * depth, depth, 2
            )
            for b in range(fs_n)
        ]
        value = jnp.concatenate(blocks, axis=2)
        return (value[0].astype(F32) + to_side(value[1]).astype(F32)).astype(BF)

    up_pair = side_block(proj_up)
    down_pair = side_block(proj_down)
    rows = after((saved_rows, upstream_grad, fresh_rows), down_pair[1])
    nears = [near_rows(r) for r in rows]
    up_whole, ups = line_gather(jnp.concatenate(up_pair, axis=0))
    saved_all = both_sides(rows[0], after(nears[0], ups[max(line_n - 2, 1)]))
    upstream_all = both_sides(rows[1], after(nears[1], ups[-1]))
    down_start = after(jnp.concatenate(down_pair, axis=0), ups[-1])
    saved_pre = jnp.dot(saved_all, up_whole, preferred_element_type=F32)
    saved_active, saved_hidden = squared_relu(saved_pre)
    down_grads = grad_scale * over_tokens(upstream_all, saved_hidden)
    down_total, _ = line_sum(down_grads)
    fresh_all = both_sides(rows[2], after(nears[2], down_grads))
    fresh_hidden = squared_relu(jnp.dot(fresh_all, up_whole, preferred_element_type=F32))[1]
    down_whole, _ = line_gather(down_start, {2: (down_grads,), 3: (fresh_hidden,)})
    hidden_grad = jnp.dot(upstream_all, down_whole, preferred_element_type=F32)
    pre_grad = (2.0 * saved_active * hidden_grad).astype(BF)
    up_grads = grad_scale * over_tokens(saved_all, pre_grad)
    fresh_hidden, pre_grad, _ = lax.optimization_barrier((fresh_hidden, pre_grad, up_grads))
    fresh_stages = share_tp(against_rows(fresh_hidden, down_whole))
    saved_stages = share_tp(against_rows(pre_grad, up_whole))
    up_total, marks = line_sum(
        up_grads, {2: (fresh_stages[0], saved_stages[0]), 3: (fresh_stages[-1],)}
    )
    middle = marks[max(line_n - 3, 0)]
    fresh_out = share_side(fresh_stages[-1])
    saved_grad = share_side(saved_stages[-1])
    down_other = after(to_side(down_total[depth:].astype(BF)), middle)
    accum_down_out = finish_grad(accum_down, down_total, down_other)
    accum_up_out = finish_grad(accum_up, up_total, to_side(up_total[depth:].astype(BF)))
    return (fresh_out, saved_grad, accum_up_out, accum_down_out)


MESH = pl.DeviceIdType.MESH
CHUNKS = 8
ROW_TILE = 512
COL_TILE = 256


def make_plan(fs_n, tp_n, row_count, width, depth, columns, chunks):
    half = columns // 2
    if tp_n != 4 or fs_n % 2 or fs_n < 6 or half % chunks or (half // chunks) % 128 or chunks < 3:
        return None
    if row_count % 64 or depth % 16 or width % COL_TILE:
        return None
    lines, tokens = fs_n // 2, 2 * row_count
    words = 5 * tokens * width + 2 * 2 * width * half + 2 * tokens * half + tokens * half // chunks
    words += 2 * (lines + 1) * 2 * depth * half + 2 * (tokens // 2 + tokens // 4 + tokens // 8) * width
    words += 2 * (tokens // 8) * width
    if 2 * words > 60 * 2**20:
        return None
    return dict(L=lines, q=row_count // 4, dp=depth, K=width, H=half, n=chunks, w=half // chunks, Tk=tokens)


def layer_kernel(plan, fresh_h, saved_h, upst_h, wu_h, wd_h, fo, so, gout,
                 rows_s, rows_u, rows_f, s_t, u_t, w, hid, pre, shid, g, gin, r1, r2, r3,
                 sem_wl, sem_wys, sem_wyr, sem_gs, sem_gr, sem_ss, sem_sr, sem_fy, sem_fyr, sem_fl,
                 sem_rl, sem_rys, sem_ryr, sem_rxs, sem_rxr, sem_rds, sem_rdr, sem_os, sem_or):
    L, q, dp, K, H, n, cw, Tk = (plan[k] for k in ("L", "q", "dp", "K", "H", "n", "w", "Tk"))
    bd = 2 * dp
    fs, tp = lax.axis_index("fs"), lax.axis_index("tp")
    z, y = fs // 2, fs % 2
    x, c0 = tp // 2, tp % 2
    not_top, not_bottom = z < L - 1, z > 0
    dev_up, dev_down = (fs + 2, tp), (fs - 2, tp)
    dev_y = (z * 2 + (1 - y), tp)
    dev_x = (fs, (1 - x) * 2 + c0)
    dev_c = (fs, x * 2 + (1 - c0))

    def remote(src, dst, send, recv, dev):
        return pltpu.make_async_remote_copy(
            src_ref=src, dst_ref=dst, send_sem=send, recv_sem=recv, device_id=dev, device_id_type=MESH)

    def al(value, size):
        return pl.multiple_of(value, size)

    barrier = pltpu.get_barrier_semaphore()

    def greet(dev):
        pl.semaphore_signal(barrier, inc=1, device_id=dev, device_id_type=MESH)

    pl.when(not_top)(lambda: greet(dev_up))
    pl.when(not_bottom)(lambda: greet(dev_down))
    greet(dev_y)
    greet(dev_x)
    greet(dev_c)
    pl.semaphore_wait(barrier, 3 + jnp.where(not_top, 1, 0) + jnp.where(not_bottom, 1, 0))

    def w_cols(c, side):
        return pl.ds(al(side * H + c * cw, 128), cw)

    w_src = (wu_h, wd_h)

    def w_local(c, p):
        return pltpu.make_async_copy(
            w_src[p].at[:, w_cols(c, y)], w.at[c, p, pl.ds(al((z * 2 + y) * dp, dp), dp), :], sem_wl.at[c, p])

    def w_side(c, p):
        return remote(
            w_src[p].at[:, w_cols(c, 1 - y)], w.at[c, p, pl.ds(al((z * 2 + y) * dp, dp), dp), :],
            sem_wys.at[c, p], sem_wyr.at[c, p], dev_y)

    def start_w(c):
        for p in range(2):
            w_side(c, p).start()
            w_local(c, p).start()

    def g_copy(c, b, way):
        part = w.at[c, :, pl.ds(al(b * bd, bd), bd), :]
        return remote(part, part, sem_gs.at[c, b, way], sem_gr.at[c, b], (dev_up, dev_down)[way])

    def g_own(c):
        for p in range(2):
            w_local(c, p).wait()
            w_side(c, p).wait_recv()
        pl.when(not_top)(lambda: g_copy(c, z, 0).start())
        pl.when(not_bottom)(lambda: g_copy(c, z, 1).start())

    def g_slot(c, s):
        low, high = z - 1 - s, z + 1 + s

        @pl.when(low >= 0)
        def _():
            g_copy(c, low, 0).wait_recv()
            pl.when(not_top)(lambda: g_copy(c, low, 0).start())

        @pl.when(high <= L - 1)
        def _():
            g_copy(c, high, 1).wait_recv()
            pl.when(not_bottom)(lambda: g_copy(c, high, 1).start())

    def block(c, b):
        return g.at[c, :, pl.ds(al(b * bd, bd), bd), :]

    def s_up(c, b):
        return remote(block(c, b), gin.at[c, b], sem_ss.at[c, b], sem_sr.at[c, b], dev_up)

    def s_down(c, b):
        return remote(block(c, b), gin.at[c, b], sem_ss.at[c, b], sem_sr.at[c, b], dev_down)

    def s_last_down(c, b):
        return remote(block(c, b), gin.at[c, L], sem_ss.at[c, b], sem_sr.at[c, L], dev_down)

    def add_in(c, b, *slots):
        for p in range(2):
            rows = pl.ds(al(b * bd, bd), bd)
            value = g[c, p, rows, :].astype(F32)
            for slot in slots:
                value = value + gin[c, slot, p].astype(F32)
            g[c, p, rows, :] = value.astype(BF)

    def s_slot(c, s):
        @pl.when((z <= s) & not_top)
        def _():
            b = L - 1 - s + z

            @pl.when(not_bottom)
            def _():
                s_up(c, b).wait_recv()
                add_in(c, b, b)

            s_up(c, b).start()

        @pl.when((L - 1 - z <= s) & not_bottom)
        def _():
            b = s - (L - 1) + z

            @pl.when(not_top)
            def _():
                s_down(c, b).wait_recv()
                add_in(c, b, b)

            if s == L - 2:
                s_last_down(c, b).start()
            else:
                s_down(c, b).start()

    def fin_side(c):
        return remote(
            g.at[c, :, pl.ds(al((z * 2 + 1 - y) * dp, dp), dp), :], gout.at[:, :, w_cols(c, y)],
            sem_fy.at[c], sem_fyr.at[c], dev_y)

    def fin_local(c):
        return pltpu.make_async_copy(
            g.at[c, :, pl.ds(al((z * 2 + y) * dp, dp), dp), :], gout.at[:, :, w_cols(c, y)], sem_fl.at[c])

    def finish(c):
        pl.when(not_bottom)(lambda: s_up(c, z).wait_recv())
        pl.when(not_top)(lambda: s_last_down(c, z).wait_recv())
        pl.when(z == 0)(lambda: add_in(c, z, L))
        pl.when(z == L - 1)(lambda: add_in(c, z, L - 1))
        pl.when(not_top & not_bottom)(lambda: add_in(c, z, z, L))
        fin_side(c).start()
        fin_local(c).start()

    row_src = (saved_h, upst_h, fresh_h)
    row_dst = (rows_s, rows_u, rows_f)

    def spot(cc, xx, yy):
        return pl.ds(al(((cc * 2 + xx) * 2 + yy) * q, q), q)

    def row_local(a, j):
        return pltpu.make_async_copy(
            row_src[a].at[pl.ds(j * q, q), :], row_dst[a].at[spot(j % 2, j // 2, y), :], sem_rl.at[a, j])

    def row_y(a):
        return remote(
            row_src[a].at[pl.ds(al(tp * q, q), q), :], row_dst[a].at[spot(c0, x, y), :],
            sem_rys.at[a], sem_ryr.at[a], dev_y)

    def row_fwd(a, xx, k, dev, send, recv):
        part = row_dst[a].at[spot(c0, xx, 1 - y), :]
        return remote(part, part, send.at[a, k], recv.at[a, k], dev)

    def x_fwd(a):
        return row_fwd(a, x, 0, dev_x, sem_rxs, sem_rxr)

    def d_fwd(a, k):
        return row_fwd(a, x if k == 0 else 1 - x, k, dev_c, sem_rds, sem_rdr)

    def rows_hop1(a):
        row_y(a).wait_recv()
        x_fwd(a).start()
        d_fwd(a, 0).start()

    def rows_hop2(a):
        x_fwd(a).wait_recv()
        d_fwd(a, 1).start()

    def rows_sent(a):
        x_fwd(a).wait_send()
        d_fwd(a, 0).wait_send()
        d_fwd(a, 1).wait_send()

    def rows_ready(a):
        for j in range(4):
            row_local(a, j).wait()
        for k in range(2):
            d_fwd(a, k).wait_recv()

    def transpose(src, dst):
        tile = COL_TILE

        def step(i, carry):
            at = pl.ds(al(i * tile, tile), tile)
            dst[at, :] = src[:, at].T
            return carry

        lax.fori_loop(0, K // tile, step, 0)

    tm = min(ROW_TILE, Tk)

    def dot(a, b):
        return jnp.dot(a, b, preferred_element_type=F32)

    def saved_part(c):
        def step(t, carry):
            r = pl.ds(al(t * tm, tm), tm)
            active = jnp.maximum(dot(rows_s[r, :], w[c, 0]), 0.0)
            shid[r, :] = (active * active).astype(BF)
            pre[c, r, :] = (2.0 * active * dot(rows_u[r, :], w[c, 1])).astype(BF)
            return carry

        lax.fori_loop(0, Tk // tm, step, 0)

        def grad(b, carry):
            r = pl.ds(al(b * bd, bd), bd)
            g[c, 0, r, :] = dot(s_t[r, :], pre[c]).astype(BF)
            g[c, 1, r, :] = dot(u_t[r, :], shid[...]).astype(BF)
            return carry

        lax.fori_loop(0, L, grad, 0)
        s_slot(c, 0)

    def fresh_part(c):
        def step(t, carry):
            r = pl.ds(al(t * tm, tm), tm)
            active = jnp.maximum(dot(rows_f[r, :], w[c, 0]), 0.0)
            hid[c, r, :] = (active * active).astype(BF)
            return carry

        lax.fori_loop(0, Tk // tm, step, 0)

    half_rows = Tk // 2

    def out_half(a, cc):
        left, stage, p = ((hid, rows_f, 1), (pre, rows_s, 0))[a]
        r = pl.ds(al(cc * half_rows, half_rows), half_rows)

        def step(d, carry):
            at = pl.ds(al(d * COL_TILE, COL_TILE), COL_TILE)
            total = None
            for c in range(n):
                term = against_rows(left[c, r, :], w[c, p, at, :])
                total = term if total is None else total + term
            stage[r, at] = total.astype(BF)
            return carry

        lax.fori_loop(0, K // COL_TILE, step, 0)

    stages = (rows_f, rows_s)
    quarter = Tk // 4

    def o1(a):
        return remote(
            stages[a].at[pl.ds(al((1 - c0) * half_rows, half_rows), half_rows), :], r1.at[a],
            sem_os.at[a, 0], sem_or.at[a, 0], dev_c)

    def o2(a):
        at = pl.ds(al(c0 * half_rows + (1 - x) * quarter, quarter), quarter)
        return remote(stages[a].at[at, :], r2.at[a], sem_os.at[a, 1], sem_or.at[a, 1], dev_x)

    def o3(a):
        return remote(stages[a].at[spot(c0, x, 1 - y), :], r3.at[a], sem_os.at[a, 2], sem_or.at[a, 2], dev_y)

    def join(a, at, *terms):
        value = stages[a][at, :].astype(F32)
        for t in terms:
            value = value + t.astype(F32)
        return value

    def out_x(a):
        o1(a).wait_recv()
        at = pl.ds(al(c0 * half_rows + (1 - x) * quarter, quarter), quarter)
        stages[a][at, :] = join(a, at, r1[a, pl.ds(al((1 - x) * quarter, quarter), quarter), :]).astype(BF)
        o2(a).start()

    def pieces(a, yy):
        return r1[a, pl.ds(al(x * quarter + yy * q, q), q), :], r2[a, pl.ds(al(yy * q, q), q), :]

    def out_y(a):
        o2(a).wait_recv()
        at = spot(c0, x, 1 - y)
        stages[a][at, :] = join(a, at, *pieces(a, 1 - y)).astype(BF)
        o3(a).start()

    def out_end(a):
        o3(a).wait_recv()
        (fo, so)[a][...] = join(a, spot(c0, x, y), *pieces(a, y), r3[a]).astype(BF)

    def period(c, first=False):
        for s in range(L - 1):
            g_slot(c, s)
            if s == 0:
                if first:
                    rows_hop1(0)
                    g_own(c + 1)
                else:
                    pl.when(c + 1 < n)(lambda: g_own(c + 1))
                    pl.when(c == 2)(lambda: rows_hop2(2))
                    pl.when(c >= 2)(lambda: mid_slots(c - 2))
            if s == L - 3:
                if first:
                    rows_hop2(0)
                    rows_hop1(1)
                else:
                    saved_part(c - 1)
                    pl.when(c == 1)(lambda: rows_hop1(2))
                    pl.when(c == 2)(lambda: rows_ready(2))
                    pl.when(c >= 2)(lambda: fresh_part(c - 2))

    def mid_slots(c):
        for s in range(1, L - 2):
            s_slot(c, s)

    def last_slot(c):
        s_slot(c, L - 2)

    start_w(0)
    row_y(0).start()
    start_w(1)
    row_y(1).start()
    for a in range(3):
        for j in range(4):
            row_local(a, j).start()
    start_w(2)
    if n > 3:
        start_w(3)
    row_y(2).start()
    for c in range(4, n):
        start_w(c)
    g_own(0)
    period(0, first=True)
    rows_ready(0)
    transpose(rows_s, s_t)
    rows_hop2(1)
    rows_ready(1)
    transpose(rows_u, u_t)
    lax.fori_loop(1, n, lambda c, carry: (period(c), carry)[1], 0)

    def over(low, high, fn):
        if high > low:
            lax.fori_loop(low, high, lambda c, carry: (fn(c), carry)[1], 0)

    early = min(2, n - 2)
    over(0, early, last_slot)
    saved_part(n - 1)
    mid_slots(n - 2)
    over(early, n - 2, last_slot)
    over(n - 2, n, fresh_part)
    for a in (0, 2):
        rows_sent(a)
    out_half(0, 1 - c0)
    o1(0).start()
    out_half(1, 1 - c0)
    o1(1).start()
    out_half(0, c0)
    out_x(0)
    out_half(1, c0)
    out_x(1)
    mid_slots(n - 1)
    last_slot(n - 2)
    over(0, n - 2, finish)
    out_y(0)
    last_slot(n - 1)
    out_y(1)
    over(n - 2, n, finish)
    out_end(0)
    out_end(1)

    def drain(c, carry):
        for p in range(2):
            w_side(c, p).wait_send()
        for b in range(L):
            pl.when((b <= z) & not_top)(lambda: g_copy(c, b, 0).wait_send())
            pl.when((b >= z) & not_bottom)(lambda: g_copy(c, b, 1).wait_send())
            pl.when(b != z)(lambda: s_up(c, b).wait_send())
        fin_side(c).wait()
        fin_local(c).wait()
        return carry

    lax.fori_loop(0, n, drain, 0)
    for a in range(3):
        row_y(a).wait_send()
    rows_sent(1)
    for a in range(2):
        o1(a).wait_send()
        o2(a).wait_send()
        o3(a).wait_send()


def fused_body(plan, fresh_rows, saved_rows, upstream_grad, proj_up, proj_down, accum_up, accum_down):
    L, q, dp, K, H, n, cw, Tk = (plan[k] for k in ("L", "q", "dp", "K", "H", "n", "w", "Tk"))
    fs_n = lax.axis_size("fs")
    grad_scale = float(fresh_rows.shape[0] * fs_n) ** (-0.5)
    dma = lambda *shape: pltpu.SemaphoreType.DMA(shape)
    vm = lambda *shape: pltpu.VMEM(shape, BF)
    flops = 2 * 6 * Tk * K * H
    any_spec = pl.BlockSpec(memory_space=pl.ANY)
    vmem_spec = pl.BlockSpec(memory_space=pltpu.VMEM)
    fresh_out, saved_grad, sums = pl.pallas_call(
        functools.partial(layer_kernel, plan),
        out_shape=(
            jax.ShapeDtypeStruct((q, K), BF),
            jax.ShapeDtypeStruct((q, K), BF),
            jax.ShapeDtypeStruct((2, dp, 2 * H), BF),
        ),
        in_specs=[any_spec] * 5,
        out_specs=(vmem_spec, vmem_spec, any_spec),
        scratch_shapes=[
            vm(Tk, K), vm(Tk, K), vm(Tk, K), vm(K, Tk), vm(K, Tk),
            vm(n, 2, K, cw), vm(n, Tk, cw), vm(n, Tk, cw), vm(Tk, cw),
            vm(n, 2, K, cw), vm(n, L + 1, 2, 2 * dp, cw),
            vm(2, Tk // 2, K), vm(2, Tk // 4, K), vm(2, q, K),
            dma(n, 2), dma(n, 2), dma(n, 2), dma(n, L, 2), dma(n, L), dma(n, L), dma(n, L + 1),
            dma(n), dma(n), dma(n),
            dma(3, 4), dma(3), dma(3), dma(3, 1), dma(3, 1), dma(3, 2), dma(3, 2), dma(2, 3), dma(2, 3),
        ],
        compiler_params=pltpu.CompilerParams(
            collective_id=0, has_side_effects=True, vmem_limit_bytes=67043328),
        cost_estimate=pl.CostEstimate(flops=flops, bytes_accessed=2**24, transcendentals=0),
    )(fresh_rows, saved_rows, upstream_grad, proj_up, proj_down)
    sums = grad_scale * sums.astype(F32)
    return fresh_out, saved_grad, accum_up + sums[0], accum_down + sums[1]


def any_body(*args):
    plan = make_plan(
        lax.axis_size("fs"), lax.axis_size("tp"), args[0].shape[0], args[0].shape[1],
        args[3].shape[0], args[3].shape[1], CHUNKS)
    if plan is None:
        return body(*args)
    return fused_body(plan, *args)


def solution(mesh):
    in_specs = (P("fs", None),) * 3 + (P("fs", "tp"),) * 4
    out_specs = (P(("fs", "tp"), None),) * 2 + (P("fs", "tp"),) * 2
    return jax.shard_map(any_body, mesh=mesh, in_specs=in_specs, out_specs=out_specs, check_vma=False)
```

```python
import functools

import jax
import jax.numpy as jnp
from jax import lax
from jax.experimental import pallas as pl
from jax.experimental.pallas import tpu as pltpu
from jax.sharding import PartitionSpec as P


BF = jnp.bfloat16
F32 = jnp.float32


def against_rows(left, right):
    return lax.dot_general(left, right, (((1,), (1,)), ((), ())), preferred_element_type=F32)


def over_tokens(left, right):
    return lax.dot_general(left, right, (((0,), (0,)), ((), ())), preferred_element_type=F32)


def squared_relu(pre_values):
    active = jnp.maximum(pre_values, 0.0)
    return (active, (active * active).astype(BF))


def after(value, *earlier):
    return lax.optimization_barrier((value, earlier))[0]


def body(fresh_rows, saved_rows, upstream_grad, proj_up, proj_down, accum_up, accum_down):
    fs_n, tp_n = lax.axis_size("fs"), lax.axis_size("tp")
    line_n = fs_n // 2
    fs, tp = lax.axis_index("fs"), lax.axis_index("tp")
    line, side = fs // 2, fs % 2
    row_count, width = fresh_rows.shape
    depth, columns = proj_up.shape
    half = columns // 2
    grad_scale = float(row_count * fs_n) ** (-0.5)

    def to_side(value):
        return lax.ppermute(value, "fs", [(i, i ^ 1) for i in range(fs_n)])

    def to_tp(value, bit):
        return lax.ppermute(value, "tp", [(j, j ^ bit) for j in range(tp_n)])

    def along(value, lines, way):
        return lax.ppermute(
            value,
            "fs",
            [(l * 2 + s, (l + way) * 2 + s) for l in lines for s in range(2)],
        )

    def side_block(weight):
        mine = lax.dynamic_slice_in_dim(weight, side * half, half, 1)
        other = lax.dynamic_slice_in_dim(weight, (1 - side) * half, half, 1)
        return mine, to_side(other)

    def line_gather(block, ties={}):
        ups, downs = [block], [block]
        for step in range(1, line_n):
            up, down = after((ups[-1], downs[-1]), *ties.get(step, ()))
            up = along(up, range(step - 1, line_n - 1), 1)
            down = along(down, range(1, line_n - step + 1), -1)
            up, down = lax.optimization_barrier((up, down))
            ups.append(up)
            downs.append(down)
        blocks = [block] + [
            jnp.where(line >= k, ups[k], downs[line_n - k]) for k in range(1, line_n)
        ]
        return jnp.concatenate(blocks, axis=0), ups

    def line_sum(grads, ties={}):
        size = 2 * depth
        up = down = None
        marks = []
        for step in range(1, line_n):
            low = grads[step * size : (step + 1) * size]
            high = grads[(line_n - step) * size : (line_n - step + 1) * size]
            low = low if up is None else low + up.astype(F32)
            high = high if down is None else high + down.astype(F32)
            low, high = after((low.astype(BF), high.astype(BF)), *ties.get(step, ()))
            up = along(low, range(0, step), 1)
            down = along(high, range(line_n - step, line_n), -1)
            up, down = lax.optimization_barrier((up, down))
            marks.append(up)
        return grads[:size] + up.astype(F32) + down.astype(F32), marks

    def finish_grad(accum, total, other):
        mine = total[:depth]
        other = other.astype(F32)
        return accum + jnp.where(
            side == 0,
            jnp.concatenate((mine, other), axis=1),
            jnp.concatenate((other, mine), axis=1),
        )

    order = [lax.rem(line - k + line_n, line_n) * 2 + (side ^ j) for k in range(line_n) for j in range(2)]
    core = tp % 2

    def near_rows(rows):
        piece = row_count // 2
        return to_side(lax.dynamic_slice_in_dim(rows, core * piece, piece, 0))

    def both_sides(rows, near):
        far = to_tp(near, 1)
        rows = jnp.concatenate(
            (rows, jnp.where(core == 0, near, far), jnp.where(core == 0, far, near)), axis=0
        )
        return jnp.concatenate(
            [lax.dynamic_slice_in_dim(rows, o * depth, depth, 1) for o in order], axis=1
        )

    def share_tp(term):
        value = term.astype(BF)
        bit, stages = 1, []
        outer = 2 * tp_n
        rest = row_count // tp_n
        value = value.reshape(2 * tp_n, rest, width)
        while bit < tp_n:
            outer //= 2
            view = value.reshape(outer, 2, rest, width)
            mine = (tp // bit) % 2
            keep = lax.dynamic_index_in_dim(view, mine, 1, keepdims=False)
            send = lax.dynamic_index_in_dim(view, 1 - mine, 1, keepdims=False)
            value = (keep.astype(F32) + to_tp(send, bit).astype(F32)).astype(BF)
            bit *= 2
            stages.append(value)
        return stages

    def share_side(value):
        blocks = [
            lax.dynamic_slice_in_dim(
                value, (lax.rem(line - b // 2 + line_n, line_n) * 2 + (side ^ (b % 2))) * depth, depth, 2
            )
            for b in range(fs_n)
        ]
        value = jnp.concatenate(blocks, axis=2)
        return (value[0].astype(F32) + to_side(value[1]).astype(F32)).astype(BF)

    up_pair = side_block(proj_up)
    down_pair = side_block(proj_down)
    rows = after((saved_rows, upstream_grad, fresh_rows), down_pair[1])
    nears = [near_rows(r) for r in rows]
    up_whole, ups = line_gather(jnp.concatenate(up_pair, axis=0))
    saved_all = both_sides(rows[0], after(nears[0], ups[max(line_n - 2, 1)]))
    upstream_all = both_sides(rows[1], after(nears[1], ups[-1]))
    down_start = after(jnp.concatenate(down_pair, axis=0), ups[-1])
    saved_pre = jnp.dot(saved_all, up_whole, preferred_element_type=F32)
    saved_active, saved_hidden = squared_relu(saved_pre)
    down_grads = grad_scale * over_tokens(upstream_all, saved_hidden)
    down_total, _ = line_sum(down_grads)
    fresh_all = both_sides(rows[2], after(nears[2], down_grads))
    fresh_hidden = squared_relu(jnp.dot(fresh_all, up_whole, preferred_element_type=F32))[1]
    down_whole, _ = line_gather(down_start, {2: (down_grads,), 3: (fresh_hidden,)})
    hidden_grad = jnp.dot(upstream_all, down_whole, preferred_element_type=F32)
    pre_grad = (2.0 * saved_active * hidden_grad).astype(BF)
    up_grads = grad_scale * over_tokens(saved_all, pre_grad)
    fresh_hidden, pre_grad, _ = lax.optimization_barrier((fresh_hidden, pre_grad, up_grads))
    fresh_stages = share_tp(against_rows(fresh_hidden, down_whole))
    saved_stages = share_tp(against_rows(pre_grad, up_whole))
    up_total, marks = line_sum(
        up_grads, {2: (fresh_stages[0], saved_stages[0]), 3: (fresh_stages[-1],)}
    )
    middle = marks[max(line_n - 3, 0)]
    fresh_out = share_side(fresh_stages[-1])
    saved_grad = share_side(saved_stages[-1])
    down_other = after(to_side(down_total[depth:].astype(BF)), middle)
    accum_down_out = finish_grad(accum_down, down_total, down_other)
    accum_up_out = finish_grad(accum_up, up_total, to_side(up_total[depth:].astype(BF)))
    return (fresh_out, saved_grad, accum_up_out, accum_down_out)


MESH = pl.DeviceIdType.MESH
CHUNKS = 8
ROW_TILE = 512
COL_TILE = 256
PIECES = 4


def make_plan(fs_n, tp_n, row_count, width, depth, columns, chunks):
    half = columns // 2
    if tp_n != 4 or fs_n % 2 or fs_n < 6 or half % chunks or (half // chunks) % 128 or chunks < 8 or chunks % 2 or fs_n < 8:
        return None
    if row_count % 128 or depth % 16 or width % (COL_TILE * PIECES):
        return None
    lines, tokens = fs_n // 2, 2 * row_count
    words = 5 * tokens * width + 2 * 2 * width * half + 2 * tokens * half + tokens * half // chunks
    words += 2 * (lines + 1) * 2 * depth * half + 2 * (tokens // 2 + tokens // 4 + tokens // 8) * width
    words += 2 * (tokens // 8) * width
    if 2 * words > 60 * 2**20:
        return None
    return dict(L=lines, q=row_count // 4, dp=depth, K=width, H=half, n=chunks, w=half // chunks, Tk=tokens)


def layer_kernel(plan, fresh_h, saved_h, upst_h, wu_h, wd_h, fo, so, gup, gdown,
                 rows_s, rows_u, rows_f, s_t, u_t, w, hid, pre, shid, g, gin, r1, r2, r3,
                 sem_wl, sem_wys, sem_wyr, sem_gs, sem_gr, sem_ss, sem_sr, sem_fy, sem_fyr, sem_fl,
                 sem_rl, sem_rys, sem_ryr, sem_rxs, sem_rxr, sem_rds, sem_rdr, sem_os, sem_or):
    L, q, dp, K, H, n, cw, Tk = (plan[k] for k in ("L", "q", "dp", "K", "H", "n", "w", "Tk"))
    bd = 2 * dp
    gouts = (gup, gdown)
    fs, tp = lax.axis_index("fs"), lax.axis_index("tp")
    z, y = fs // 2, fs % 2
    x, c0 = tp // 2, tp % 2
    not_top, not_bottom = z < L - 1, z > 0
    dev_up, dev_down = (fs + 2, tp), (fs - 2, tp)
    dev_y = (z * 2 + (1 - y), tp)
    dev_x = (fs, (1 - x) * 2 + c0)
    dev_c = (fs, x * 2 + (1 - c0))

    def remote(src, dst, send, recv, dev):
        return pltpu.make_async_remote_copy(
            src_ref=src, dst_ref=dst, send_sem=send, recv_sem=recv, device_id=dev, device_id_type=MESH)

    def al(value, size):
        return pl.multiple_of(value, size)

    barrier = pltpu.get_barrier_semaphore()

    def greet(dev):
        pl.semaphore_signal(barrier, inc=1, device_id=dev, device_id_type=MESH)

    pl.when(not_top)(lambda: greet(dev_up))
    pl.when(not_bottom)(lambda: greet(dev_down))
    greet(dev_y)
    greet(dev_x)
    greet(dev_c)
    pl.semaphore_wait(barrier, 3 + jnp.where(not_top, 1, 0) + jnp.where(not_bottom, 1, 0))

    def w_cols(c, side):
        return pl.ds(al(side * H + c * cw, 128), cw)

    w_src = (wu_h, wd_h)

    def w_local(c, p):
        return pltpu.make_async_copy(
            w_src[p].at[:, w_cols(c, y)], w.at[c, p, pl.ds(al((z * 2 + y) * dp, dp), dp), :], sem_wl.at[c, p])

    def w_side(c, p):
        return remote(
            w_src[p].at[:, w_cols(c, 1 - y)], w.at[c, p, pl.ds(al((z * 2 + y) * dp, dp), dp), :],
            sem_wys.at[c, p], sem_wyr.at[c, p], dev_y)

    def start_w(c):
        for p in range(2):
            w_side(c, p).start()
            w_local(c, p).start()

    def g_copy(c, b, way):
        part = w.at[c, :, pl.ds(al(b * bd, bd), bd), :]
        return remote(part, part, sem_gs.at[c, b, way], sem_gr.at[c, b], (dev_up, dev_down)[way])

    def g_ready(c):
        for p in range(2):
            w_local(c, p).wait()
            w_side(c, p).wait_recv()

    def g_first():
        def part(side):
            rows = w.at[0, :, pl.ds(al((z * 2 + side) * dp, dp), dp), :]

            def send(way):
                remote(rows, rows, sem_gs.at[0, z, way], sem_gr.at[0, z], (dev_up, dev_down)[way]).start()

            pl.when(not_top)(lambda: send(0))
            pl.when(not_bottom)(lambda: send(1))

        for p in range(2):
            w_local(0, p).wait()
        part(y)
        for p in range(2):
            w_side(0, p).wait_recv()
        part(1 - y)

    def by_lead(lead, up, down):
        leads = range(lead, L - 1) if lead == 2 else (lead,)
        for a in leads:
            pl.when(z == L - 2 - a)(up)
            pl.when(z == 1 + a)(down)

    def g_own(lead, c):
        by_lead(lead, lambda: g_copy(c, z, 0).start(), lambda: g_copy(c, z, 1).start())

    def s_last(lead, c):
        by_lead(lead, lambda: s_slot_up(c, L - 2), lambda: s_slot_down(c, L - 2))

    at_end = (z == 0) | (z == L - 1)

    def g_low(c, s):
        low = z - 1 - s

        @pl.when(low >= 0)
        def _():
            g_copy(c, low, 0).wait_recv()
            pl.when(not_top)(lambda: g_copy(c, low, 0).start())

    def g_high(c, s):
        high = z + 1 + s

        @pl.when(high <= L - 1)
        def _():
            g_copy(c, high, 1).wait_recv()
            pl.when(not_bottom)(lambda: g_copy(c, high, 1).start())

    def g_slot(c, s):
        g_low(c, s)
        g_high(c, s)

    def g_lead(c):
        for ahead in range(1, L - 2):
            for k in range(ahead):
                for s in range(L - 2 - ahead):
                    pl.when(z == L - 2 - ahead)(lambda: g_low(c + k, s))
                    pl.when(z == 1 + ahead)(lambda: g_high(c + k, s))

    def g_slot_ahead(c, s):
        for ahead in range(L - 2):
            fits = c + ahead < n
            pl.when((z == L - 2 - ahead) & fits)(lambda: g_low(c + ahead, s))
            pl.when((z == 1 + ahead) & fits)(lambda: g_high(c + ahead, s))
        pl.when(z == L - 1)(lambda: g_low(c, s))
        pl.when(z == 0)(lambda: g_high(c, s))

    def block(c, b):
        return g.at[c, :, pl.ds(al(b * bd, bd), bd), :]

    def s_up(c, b):
        return remote(block(c, b), gin.at[c, b], sem_ss.at[c, b], sem_sr.at[c, b], dev_up)

    def s_down(c, b):
        return remote(block(c, b), gin.at[c, b], sem_ss.at[c, b], sem_sr.at[c, b], dev_down)

    def s_last_down(c, b):
        return remote(block(c, b), gin.at[c, L], sem_ss.at[c, b], sem_sr.at[c, L], dev_down)

    def add_in(c, b, *slots):
        for p in range(2):
            rows = pl.ds(al(b * bd, bd), bd)
            value = g[c, p, rows, :].astype(F32)
            for slot in slots:
                value = value + gin[c, slot, p].astype(F32)
            g[c, p, rows, :] = value.astype(BF)

    def s_slot_up(c, s):
        @pl.when((z <= s) & not_top)
        def _():
            b = L - 1 - s + z

            @pl.when(not_bottom)
            def _():
                s_up(c, b).wait_recv()
                add_in(c, b, b)

            s_up(c, b).start()

    def s_slot_down(c, s):
        @pl.when((L - 1 - z <= s) & not_bottom)
        def _():
            b = s - (L - 1) + z

            @pl.when(not_top)
            def _():
                s_down(c, b).wait_recv()
                add_in(c, b, b)

            if s == L - 2:
                s_last_down(c, b).start()
            else:
                s_down(c, b).start()

    def s_slot(c, s):
        s_slot_up(c, s)
        s_slot_down(c, s)

    def fin_side(c, p):
        return remote(
            g.at[c, p, pl.ds(al((z * 2 + 1 - y) * dp, dp), dp), :], gouts[p].at[:, w_cols(c, y)],
            sem_fy.at[c, p], sem_fyr.at[c, p], dev_y)

    def fin_local(c, p):
        return pltpu.make_async_copy(
            g.at[c, p, pl.ds(al((z * 2 + y) * dp, dp), dp), :], gouts[p].at[:, w_cols(c, y)], sem_fl.at[c, p])

    def finish(c):
        pl.when(not_bottom)(lambda: s_up(c, z).wait_recv())
        pl.when(not_top)(lambda: s_last_down(c, z).wait_recv())
        pl.when(z == 0)(lambda: add_in(c, z, L))
        pl.when(z == L - 1)(lambda: add_in(c, z, L - 1))
        pl.when(not_top & not_bottom)(lambda: add_in(c, z, z, L))
        for p in range(2):
            fin_side(c, p).start()
            fin_local(c, p).start()

    row_src = (saved_h, upst_h, fresh_h)
    row_dst = (rows_s, rows_u, rows_f)

    def spot(cc, xx, yy):
        return pl.ds(al(((cc * 2 + xx) * 2 + yy) * q, q), q)

    def row_local(a, j):
        return pltpu.make_async_copy(
            row_src[a].at[pl.ds(j * q, q), :], row_dst[a].at[spot(j % 2, j // 2, y), :], sem_rl.at[a, j])

    half_q = q // 2

    def spot_piece(cc, xx, yy, k):
        return pl.ds(al(((cc * 2 + xx) * 2 + yy) * q + k * half_q, half_q), half_q)

    def row_y(a, k):
        return remote(
            row_src[a].at[pl.ds(al(tp * q + k * half_q, half_q), half_q), :],
            row_dst[a].at[spot_piece(c0, x, y, k), :], sem_rys.at[a, k], sem_ryr.at[a, k], dev_y)

    def row_start(a):
        for k in range(2):
            row_y(a, k).start()

    def x_fwd(a, k):
        part = row_dst[a].at[spot_piece(c0, x, 1 - y, k), :]
        return remote(part, part, sem_rxs.at[a, k], sem_rxr.at[a, k], dev_x)

    def d_fwd(a, k):
        part = row_dst[a].at[spot(c0, x if k == 0 else 1 - x, 1 - y), :]
        return remote(part, part, sem_rds.at[a, k], sem_rdr.at[a, k], dev_c)

    def rows_hop1(a, k):
        row_y(a, k).wait_recv()
        x_fwd(a, k).start()
        if k == 1:
            d_fwd(a, 0).start()

    def rows_hop2(a):
        for k in range(2):
            x_fwd(a, k).wait_recv()
        d_fwd(a, 1).start()

    def rows_sent(a):
        for k in range(2):
            x_fwd(a, k).wait_send()
        d_fwd(a, 0).wait_send()
        d_fwd(a, 1).wait_send()

    def rows_ready(a):
        for j in range(4):
            row_local(a, j).wait()
        for k in range(2):
            d_fwd(a, k).wait_recv()

    def transpose(src, dst):
        tile = COL_TILE

        def step(i, carry):
            at = pl.ds(al(i * tile, tile), tile)
            dst[at, :] = src[:, at].T
            return carry

        lax.fori_loop(0, K // tile, step, 0)

    tm = min(ROW_TILE, Tk)

    def dot(a, b):
        return jnp.dot(a, b, preferred_element_type=F32)

    def saved_part(c):
        def step(t, carry):
            r = pl.ds(al(t * tm, tm), tm)
            active = jnp.maximum(dot(rows_s[r, :], w[c, 0]), 0.0)
            shid[r, :] = (active * active).astype(BF)
            pre[c, r, :] = (2.0 * active * dot(rows_u[r, :], w[c, 1])).astype(BF)
            return carry

        lax.fori_loop(0, Tk // tm, step, 0)

        def grad(b, carry):
            r = pl.ds(al(b * bd, bd), bd)
            g[c, 0, r, :] = dot(s_t[r, :], pre[c]).astype(BF)
            g[c, 1, r, :] = dot(u_t[r, :], shid[...]).astype(BF)
            return carry

        lax.fori_loop(0, L, grad, 0)
        s_slot(c, 0)

    def fresh_part(c):
        def step(t, carry):
            r = pl.ds(al(t * tm, tm), tm)
            active = jnp.maximum(dot(rows_f[r, :], w[c, 0]), 0.0)
            hid[c, r, :] = (active * active).astype(BF)
            return carry

        lax.fori_loop(0, Tk // tm, step, 0)

    half_rows = Tk // 2

    pw = K // PIECES

    def out_piece(a, cc, h):
        left, stage, p = ((hid, rows_f, 1), (pre, rows_s, 0))[a]
        r = pl.ds(al(cc * half_rows, half_rows), half_rows)

        def step(d, carry):
            at = pl.ds(al(h * pw + d * COL_TILE, COL_TILE), COL_TILE)
            total = None
            for c in range(0, n, 2):
                term = against_rows(
                    jnp.concatenate((left[c, r, :], left[c + 1, r, :]), axis=1),
                    jnp.concatenate((w[c, p, at, :], w[c + 1, p, at, :]), axis=1))
                total = term if total is None else total + term
            stage[r, at] = total.astype(BF)
            return carry

        lax.fori_loop(0, pw // COL_TILE, step, 0)

    stages = (rows_f, rows_s)
    quarter = Tk // 4
    far_x = pl.ds(al(c0 * half_rows + (1 - x) * quarter, quarter), quarter)

    def cols(h):
        return pl.ds(h * pw, pw)

    def o1(a, h):
        return remote(
            stages[a].at[pl.ds(al((1 - c0) * half_rows, half_rows), half_rows), cols(h)], r1.at[a, :, cols(h)],
            sem_os.at[a, 0, h], sem_or.at[a, 0, h], dev_c)

    def o2(a, h):
        return remote(
            stages[a].at[far_x, cols(h)], r2.at[a, :, cols(h)], sem_os.at[a, 1, h], sem_or.at[a, 1, h], dev_x)

    def o3(a, h):
        return remote(
            stages[a].at[spot(c0, x, 1 - y), cols(h)], r3.at[a, :, cols(h)],
            sem_os.at[a, 2, h], sem_or.at[a, 2, h], dev_y)

    def join(a, at, h, *terms):
        value = stages[a][at, cols(h)].astype(F32)
        for t in terms:
            value = value + t.astype(F32)
        return value

    def out_c(a, h):
        out_piece(a, 1 - c0, h)
        o1(a, h).start()

    def out_x(a, h):
        out_piece(a, c0, h)
        o1(a, h).wait_recv()
        part = r1[a, pl.ds(al((1 - x) * quarter, quarter), quarter), cols(h)]
        stages[a][far_x, cols(h)] = join(a, far_x, h, part).astype(BF)
        o2(a, h).start()

    def out_pair(a, h):
        out_c(a, h)
        out_c(a, h + 1)
        out_x(a, h)
        out_x(a, h + 1)

    def pieces(a, yy, h):
        return (r1[a, pl.ds(al(x * quarter + yy * q, q), q), cols(h)],
                r2[a, pl.ds(al(yy * q, q), q), cols(h)])

    def out_y(a, h):
        o2(a, h).wait_recv()
        at = spot(c0, x, 1 - y)
        stages[a][at, cols(h)] = join(a, at, h, *pieces(a, 1 - y, h)).astype(BF)
        o3(a, h).start()

    def out_end(a, h):
        o3(a, h).wait_recv()
        (fo, so)[a][:, cols(h)] = join(
            a, spot(c0, x, y), h, *pieces(a, y, h), r3[a, :, cols(h)]).astype(BF)

    def mid_slots(c):
        for s in range(1, L - 2):
            s_slot(c, s)

    def over(low, high, fn):
        if high > low:
            lax.fori_loop(low, high, lambda c, carry: (fn(c), carry)[1], 0)

    middle = range(1, L - 2)
    start_w(0)
    start_w(1)
    row_y(0, 0).start()
    start_w(2)
    row_y(0, 1).start()
    start_w(3)
    row_y(1, 0).start()
    row_y(1, 1).start()
    for a in range(3):
        for j in range(4):
            row_local(a, j).start()
    over(4, n, start_w)
    row_y(2, 0).start()
    row_y(2, 1).start()

    g_first()
    g_ready(1)
    g_own(2, 1)
    g_slot(0, 0)
    g_own(1, 1)
    rows_hop1(0, 0)
    g_ready(2)
    g_own(2, 2)
    for s in middle:
        g_slot(0, s)
    g_own(0, 1)
    rows_hop1(0, 1)
    g_slot(0, L - 2)
    g_own(1, 2)
    g_ready(3)
    g_own(2, 3)
    rows_hop2(0)
    g_slot(1, 0)
    g_own(1, 3)
    rows_hop1(1, 0)
    rows_ready(0)
    transpose(rows_s, s_t)
    g_own(0, 2)
    for s in middle:
        g_slot(1, s)
    rows_hop1(1, 1)
    g_ready(4)
    g_own(2, 4)
    g_own(1, 4)
    rows_hop2(1)
    g_slot(1, L - 2)
    g_ready(5)
    g_own(2, 5)
    rows_ready(1)
    transpose(rows_u, u_t)
    g_lead(2)
    g_slot_ahead(2, 0)
    g_own(0, 3)
    g_own(1, 5)
    saved_part(0)
    over(6, n, g_ready)
    over(6, n, lambda c: g_own(2, c))
    g_own(1, 6)
    for s in middle:
        g_slot_ahead(2, s)
    saved_part(1)
    g_slot_ahead(2, L - 2)
    rows_hop1(2, 0)
    rows_hop1(2, 1)
    g_slot_ahead(3, 0)
    g_own(0, 4)
    over(7, n, lambda c: g_own(1, c))
    for s in middle:
        g_slot_ahead(3, s)
    saved_part(2)
    mid_slots(0)
    rows_hop2(2)
    g_slot_ahead(3, L - 2)
    rows_ready(2)
    over(0, 3, fresh_part)
    mid_slots(1)

    def period(c):
        g_slot_ahead(c, 0)
        pl.when(c + 1 < n)(lambda: g_own(0, c + 1))
        for s in middle:
            g_slot_ahead(c, s)
        saved_part(c - 1)
        fresh_part(c - 1)
        mid_slots(c - 2)
        s_last(2, c - 4)
        pl.when(c >= 5)(lambda: s_last(1, c - 5))
        g_slot_ahead(c, L - 2)

    over(4, n, period)

    over(0, n - 3, lambda c: s_last(0, c))
    s_last(1, n - 5)
    fresh_part(n - 1)
    for a in (0, 2):
        rows_sent(a)
    out_c(0, 0)
    out_c(0, 1)
    out_x(0, 0)
    out_x(0, 1)
    mid_slots(n - 2)
    s_last(0, n - 3)
    saved_part(n - 1)
    pl.when(at_end)(lambda: mid_slots(n - 1))
    over(n - 4, n - 1, lambda c: s_last(2, c))
    out_c(0, 2)
    out_c(0, 3)
    out_x(0, 2)
    finish(0)
    out_x(0, 3)
    out_y(0, 0)
    finish(1)
    out_c(1, 0)
    out_c(1, 1)
    out_x(1, 0)
    pl.when(jnp.logical_not(at_end))(lambda: mid_slots(n - 1))
    s_last(0, n - 2)
    over(n - 4, n - 1, lambda c: s_last(1, c))
    out_y(0, 1)
    finish(2)
    out_x(1, 1)
    out_c(1, 2)
    out_c(1, 3)
    out_x(1, 2)
    finish(3)
    out_x(1, 3)
    out_y(0, 2)
    s_last(2, n - 1)
    s_last(1, n - 1)
    out_y(0, 3)
    over(4, n - 3, finish)
    s_last(0, n - 1)
    out_y(1, 0)
    finish(n - 3)
    out_y(1, 1)
    out_end(0, 0)
    out_end(0, 1)
    pl.when(at_end)(lambda: finish(n - 2))
    out_y(1, 2)
    pl.when(jnp.logical_not(at_end))(lambda: finish(n - 2))
    out_end(0, 2)
    out_end(0, 3)
    pl.when(at_end)(lambda: finish(n - 1))
    out_y(1, 3)
    pl.when(jnp.logical_not(at_end))(lambda: finish(n - 1))
    for h in range(PIECES):
        out_end(1, h)

    def drain(c, carry):
        for p in range(2):
            w_side(c, p).wait_send()
            fin_side(c, p).wait()
            fin_local(c, p).wait()
        for b in range(L):
            pl.when((b <= z) & not_top)(lambda: g_copy(c, b, 0).wait_send())
            pl.when((b >= z) & not_bottom)(lambda: g_copy(c, b, 1).wait_send())
            pl.when(b != z)(lambda: s_up(c, b).wait_send())
        return carry

    lax.fori_loop(0, n, drain, 0)
    for a in range(3):
        for k in range(2):
            row_y(a, k).wait_send()
    rows_sent(1)
    for a in range(2):
        for h in range(PIECES):
            o1(a, h).wait_send()
        for h in range(PIECES):
            o2(a, h).wait_send()
            o3(a, h).wait_send()


def finish_kernel(grad_scale, fresh_in, saved_in, up_in, down_in, up_sum, down_sum, fresh, saved, up, down):
    fresh[...] = fresh_in[...]
    saved[...] = saved_in[...]
    up[...] = up_in[...] + grad_scale * up_sum[...].astype(F32)
    down[...] = down_in[...] + grad_scale * down_sum[...].astype(F32)


def finish_call(grad_scale, *arrays):
    steps = 4

    def spec(a):
        return pl.BlockSpec((a.shape[0] // steps, a.shape[1]), lambda i: (i, 0))

    outs = arrays[:4]
    return pl.pallas_call(
        functools.partial(finish_kernel, grad_scale),
        grid=(steps,),
        in_specs=[spec(a) for a in arrays],
        out_specs=[spec(a) for a in outs],
        out_shape=[jax.ShapeDtypeStruct(a.shape, a.dtype) for a in outs],
        cost_estimate=pl.CostEstimate(flops=2**20, bytes_accessed=2**24, transcendentals=0),
    )(*arrays)


def fused_body(plan, fresh_rows, saved_rows, upstream_grad, proj_up, proj_down, accum_up, accum_down):
    L, q, dp, K, H, n, cw, Tk = (plan[k] for k in ("L", "q", "dp", "K", "H", "n", "w", "Tk"))
    fs_n = lax.axis_size("fs")
    grad_scale = float(fresh_rows.shape[0] * fs_n) ** (-0.5)
    dma = lambda *shape: pltpu.SemaphoreType.DMA(shape)
    vm = lambda *shape: pltpu.VMEM(shape, BF)
    flops = 2 * 6 * Tk * K * H
    any_spec = pl.BlockSpec(memory_space=pl.ANY)
    vmem_spec = pl.BlockSpec(memory_space=pltpu.VMEM)
    fresh_out, saved_grad, up_sum, down_sum = pl.pallas_call(
        functools.partial(layer_kernel, plan),
        out_shape=(
            jax.ShapeDtypeStruct((q, K), BF),
            jax.ShapeDtypeStruct((q, K), BF),
            jax.ShapeDtypeStruct((dp, 2 * H), BF),
            jax.ShapeDtypeStruct((dp, 2 * H), BF),
        ),
        in_specs=[any_spec] * 5,
        out_specs=(vmem_spec, vmem_spec, any_spec, any_spec),
        scratch_shapes=[
            vm(Tk, K), vm(Tk, K), vm(Tk, K), vm(K, Tk), vm(K, Tk),
            vm(n, 2, K, cw), vm(n, Tk, cw), vm(n, Tk, cw), vm(Tk, cw),
            vm(n, 2, K, cw), vm(n, L + 1, 2, 2 * dp, cw),
            vm(2, Tk // 2, K), vm(2, Tk // 4, K), vm(2, q, K),
            dma(n, 2), dma(n, 2), dma(n, 2), dma(n, L, 2), dma(n, L), dma(n, L), dma(n, L + 1),
            dma(n, 2), dma(n, 2), dma(n, 2),
            dma(3, 4), dma(3, 2), dma(3, 2), dma(3, 2), dma(3, 2), dma(3, 2), dma(3, 2), dma(2, 3, PIECES), dma(2, 3, PIECES),
        ],
        compiler_params=pltpu.CompilerParams(
            collective_id=0, has_side_effects=True, vmem_limit_bytes=67043328),
        cost_estimate=pl.CostEstimate(flops=flops, bytes_accessed=2**24, transcendentals=0),
    )(fresh_rows, saved_rows, upstream_grad, proj_up, proj_down)
    return finish_call(grad_scale, fresh_out, saved_grad, accum_up, accum_down, up_sum, down_sum)


def any_body(*args):
    plan = make_plan(
        lax.axis_size("fs"), lax.axis_size("tp"), args[0].shape[0], args[0].shape[1],
        args[3].shape[0], args[3].shape[1], CHUNKS)
    if plan is None:
        return body(*args)
    return fused_body(plan, *args)


def solution(mesh):
    in_specs = (P("fs", None),) * 3 + (P("fs", "tp"),) * 4
    out_specs = (P(("fs", "tp"), None),) * 2 + (P("fs", "tp"),) * 2
    return jax.shard_map(any_body, mesh=mesh, in_specs=in_specs, out_specs=out_specs, check_vma=False)
```

```python
import functools

import jax
import jax.numpy as jnp
from jax import lax
from jax.experimental import pallas as pl
from jax.experimental.pallas import tpu as pltpu
from jax.sharding import PartitionSpec as P


BF = jnp.bfloat16
F32 = jnp.float32


def against_rows(left, right):
    return lax.dot_general(left, right, (((1,), (1,)), ((), ())), preferred_element_type=F32)


def over_tokens(left, right):
    return lax.dot_general(left, right, (((0,), (0,)), ((), ())), preferred_element_type=F32)


def squared_relu(pre_values):
    active = jnp.maximum(pre_values, 0.0)
    return (active, (active * active).astype(BF))


def after(value, *earlier):
    return lax.optimization_barrier((value, earlier))[0]


def body(fresh_rows, saved_rows, upstream_grad, proj_up, proj_down, accum_up, accum_down):
    fs_n, tp_n = lax.axis_size("fs"), lax.axis_size("tp")
    line_n = fs_n // 2
    fs, tp = lax.axis_index("fs"), lax.axis_index("tp")
    line, side = fs // 2, fs % 2
    row_count, width = fresh_rows.shape
    depth, columns = proj_up.shape
    half = columns // 2
    grad_scale = float(row_count * fs_n) ** (-0.5)

    def to_side(value):
        return lax.ppermute(value, "fs", [(i, i ^ 1) for i in range(fs_n)])

    def to_tp(value, bit):
        return lax.ppermute(value, "tp", [(j, j ^ bit) for j in range(tp_n)])

    def along(value, lines, way):
        return lax.ppermute(
            value,
            "fs",
            [(l * 2 + s, (l + way) * 2 + s) for l in lines for s in range(2)],
        )

    def side_block(weight):
        mine = lax.dynamic_slice_in_dim(weight, side * half, half, 1)
        other = lax.dynamic_slice_in_dim(weight, (1 - side) * half, half, 1)
        return mine, to_side(other)

    def line_gather(block, ties={}):
        ups, downs = [block], [block]
        for step in range(1, line_n):
            up, down = after((ups[-1], downs[-1]), *ties.get(step, ()))
            up = along(up, range(step - 1, line_n - 1), 1)
            down = along(down, range(1, line_n - step + 1), -1)
            up, down = lax.optimization_barrier((up, down))
            ups.append(up)
            downs.append(down)
        blocks = [block] + [
            jnp.where(line >= k, ups[k], downs[line_n - k]) for k in range(1, line_n)
        ]
        return jnp.concatenate(blocks, axis=0), ups

    def line_sum(grads, ties={}):
        size = 2 * depth
        up = down = None
        marks = []
        for step in range(1, line_n):
            low = grads[step * size : (step + 1) * size]
            high = grads[(line_n - step) * size : (line_n - step + 1) * size]
            low = low if up is None else low + up.astype(F32)
            high = high if down is None else high + down.astype(F32)
            low, high = after((low.astype(BF), high.astype(BF)), *ties.get(step, ()))
            up = along(low, range(0, step), 1)
            down = along(high, range(line_n - step, line_n), -1)
            up, down = lax.optimization_barrier((up, down))
            marks.append(up)
        return grads[:size] + up.astype(F32) + down.astype(F32), marks

    def finish_grad(accum, total, other):
        mine = total[:depth]
        other = other.astype(F32)
        return accum + jnp.where(
            side == 0,
            jnp.concatenate((mine, other), axis=1),
            jnp.concatenate((other, mine), axis=1),
        )

    order = [lax.rem(line - k + line_n, line_n) * 2 + (side ^ j) for k in range(line_n) for j in range(2)]
    core = tp % 2

    def near_rows(rows):
        piece = row_count // 2
        return to_side(lax.dynamic_slice_in_dim(rows, core * piece, piece, 0))

    def both_sides(rows, near):
        far = to_tp(near, 1)
        rows = jnp.concatenate(
            (rows, jnp.where(core == 0, near, far), jnp.where(core == 0, far, near)), axis=0
        )
        return jnp.concatenate(
            [lax.dynamic_slice_in_dim(rows, o * depth, depth, 1) for o in order], axis=1
        )

    def share_tp(term):
        value = term.astype(BF)
        bit, stages = 1, []
        outer = 2 * tp_n
        rest = row_count // tp_n
        value = value.reshape(2 * tp_n, rest, width)
        while bit < tp_n:
            outer //= 2
            view = value.reshape(outer, 2, rest, width)
            mine = (tp // bit) % 2
            keep = lax.dynamic_index_in_dim(view, mine, 1, keepdims=False)
            send = lax.dynamic_index_in_dim(view, 1 - mine, 1, keepdims=False)
            value = (keep.astype(F32) + to_tp(send, bit).astype(F32)).astype(BF)
            bit *= 2
            stages.append(value)
        return stages

    def share_side(value):
        blocks = [
            lax.dynamic_slice_in_dim(
                value, (lax.rem(line - b // 2 + line_n, line_n) * 2 + (side ^ (b % 2))) * depth, depth, 2
            )
            for b in range(fs_n)
        ]
        value = jnp.concatenate(blocks, axis=2)
        return (value[0].astype(F32) + to_side(value[1]).astype(F32)).astype(BF)

    up_pair = side_block(proj_up)
    down_pair = side_block(proj_down)
    rows = after((saved_rows, upstream_grad, fresh_rows), down_pair[1])
    nears = [near_rows(r) for r in rows]
    up_whole, ups = line_gather(jnp.concatenate(up_pair, axis=0))
    saved_all = both_sides(rows[0], after(nears[0], ups[max(line_n - 2, 1)]))
    upstream_all = both_sides(rows[1], after(nears[1], ups[-1]))
    down_start = after(jnp.concatenate(down_pair, axis=0), ups[-1])
    saved_pre = jnp.dot(saved_all, up_whole, preferred_element_type=F32)
    saved_active, saved_hidden = squared_relu(saved_pre)
    down_grads = grad_scale * over_tokens(upstream_all, saved_hidden)
    down_total, _ = line_sum(down_grads)
    fresh_all = both_sides(rows[2], after(nears[2], down_grads))
    fresh_hidden = squared_relu(jnp.dot(fresh_all, up_whole, preferred_element_type=F32))[1]
    down_whole, _ = line_gather(down_start, {2: (down_grads,), 3: (fresh_hidden,)})
    hidden_grad = jnp.dot(upstream_all, down_whole, preferred_element_type=F32)
    pre_grad = (2.0 * saved_active * hidden_grad).astype(BF)
    up_grads = grad_scale * over_tokens(saved_all, pre_grad)
    fresh_hidden, pre_grad, _ = lax.optimization_barrier((fresh_hidden, pre_grad, up_grads))
    fresh_stages = share_tp(against_rows(fresh_hidden, down_whole))
    saved_stages = share_tp(against_rows(pre_grad, up_whole))
    up_total, marks = line_sum(
        up_grads, {2: (fresh_stages[0], saved_stages[0]), 3: (fresh_stages[-1],)}
    )
    middle = marks[max(line_n - 3, 0)]
    fresh_out = share_side(fresh_stages[-1])
    saved_grad = share_side(saved_stages[-1])
    down_other = after(to_side(down_total[depth:].astype(BF)), middle)
    accum_down_out = finish_grad(accum_down, down_total, down_other)
    accum_up_out = finish_grad(accum_up, up_total, to_side(up_total[depth:].astype(BF)))
    return (fresh_out, saved_grad, accum_up_out, accum_down_out)


MESH = pl.DeviceIdType.MESH
CHUNKS = 8
ROW_TILE = 512
COL_TILE = 256
PIECES = 4


def make_plan(fs_n, tp_n, row_count, width, depth, columns, chunks):
    half = columns // 2
    if tp_n != 4 or fs_n % 2 or fs_n < 6 or half % chunks or (half // chunks) % 128 or chunks < 8 or chunks % 2 or fs_n < 8:
        return None
    if row_count % 128 or depth % 16 or width % (COL_TILE * PIECES):
        return None
    lines, tokens = fs_n // 2, 2 * row_count
    words = 5 * tokens * width + 2 * 2 * width * half + 2 * tokens * half + tokens * half // chunks
    words += 2 * (lines + 1) * 2 * depth * half + 2 * (tokens // 2 + tokens // 4 + tokens // 8) * width
    words += 2 * (tokens // 8) * width
    if 2 * words > 60 * 2**20:
        return None
    return dict(L=lines, q=row_count // 4, dp=depth, K=width, H=half, n=chunks, w=half // chunks, Tk=tokens)


def layer_kernel(plan, fresh_h, saved_h, upst_h, wu_h, wd_h, fo, so, gup, gdown,
                 rows_s, rows_u, rows_f, s_t, u_t, w, hid, pre, shid, g, gin, r1, r2, r3,
                 sem_wl, sem_wys, sem_wyr, sem_gs, sem_gr, sem_ss, sem_sr, sem_fy, sem_fyr, sem_fl,
                 sem_rl, sem_rys, sem_ryr, sem_rs, sem_rxr, sem_rdr, sem_os, sem_or, sem_ol):
    L, q, dp, K, H, n, cw, Tk = (plan[k] for k in ("L", "q", "dp", "K", "H", "n", "w", "Tk"))
    bd = 2 * dp
    gouts = (gup, gdown)
    fs, tp = lax.axis_index("fs"), lax.axis_index("tp")
    z, y = fs // 2, fs % 2
    x, c0 = tp // 2, tp % 2
    not_top, not_bottom = z < L - 1, z > 0
    dev_up, dev_down = (fs + 2, tp), (fs - 2, tp)
    dev_y = (z * 2 + (1 - y), tp)
    dev_x = (fs, (1 - x) * 2 + c0)
    dev_c = (fs, x * 2 + (1 - c0))

    def remote(src, dst, send, recv, dev):
        return pltpu.make_async_remote_copy(
            src_ref=src, dst_ref=dst, send_sem=send, recv_sem=recv, device_id=dev, device_id_type=MESH)

    def all_sent(ref, sem):
        pltpu.make_async_copy(ref, ref, sem).wait()

    def al(value, size):
        return pl.multiple_of(value, size)

    barrier = pltpu.get_barrier_semaphore()

    def greet(dev):
        pl.semaphore_signal(barrier, inc=1, device_id=dev, device_id_type=MESH)

    def w_cols(c, side):
        return pl.ds(al(side * H + c * cw, 128), cw)

    w_src = (wu_h, wd_h)
    my_rows = pl.ds(al((z * 2 + y) * dp, dp), dp)
    side_rows = pl.ds(al((z * 2 + 1 - y) * dp, dp), dp)

    def w_local(c, p):
        return pltpu.make_async_copy(
            w_src[p].at[:, w_cols(c, y)], w.at[c, p, my_rows, :], sem_wl.at[jnp.where(c < 2, 0, 1)])

    def w_side(c, p):
        return remote(
            w_src[p].at[:, w_cols(c, 1 - y)], w.at[c, p, my_rows, :], sem_wys, sem_wyr.at[c], dev_y)

    def start_w(c):
        for p in range(2):
            w_side(c, p).start()

    def w_start_local(c):
        for p in range(2):
            w_local(c, p).start()

    def g_copy(c, b, way):
        part = w.at[c, :, pl.ds(al(b * bd, bd), bd), :]
        return remote(part, part, sem_gs.at[way], sem_gr.at[c, b], (dev_up, dev_down)[way])

    def g_local(low, high):
        all_sent(w.at[low:high, :, my_rows, :], sem_wl.at[0 if low == 0 else 1])

    def g_side(c):
        all_sent(w.at[c, :, side_rows, :], sem_wyr.at[c])

    def by_lead(lead, up, down):
        leads = range(lead, L - 1) if lead == 2 else (lead,)
        for a in leads:
            pl.when(z == L - 2 - a)(up)
            pl.when(z == 1 + a)(down)

    def g_part(c, side, way):
        rows = w.at[c, :, pl.ds(al((z * 2 + side) * dp, dp), dp), :]
        remote(rows, rows, sem_gs.at[way], sem_gr.at[c, z], (dev_up, dev_down)[way]).start()

    def g_near(lead, c):
        by_lead(lead, lambda: g_part(c, y, 0), lambda: g_part(c, y, 1))

    def g_far(lead, c):
        by_lead(lead, lambda: g_part(c, 1 - y, 0), lambda: g_part(c, 1 - y, 1))

    def g_own(lead, c):
        g_near(lead, c)
        g_far(lead, c)

    def s_last(lead, c):
        by_lead(lead, lambda: s_slot_up(c, L - 2), lambda: s_slot_down(c, L - 2))

    at_end = (z == 0) | (z == L - 1)

    def g_low(c, s):
        low = z - 1 - s

        @pl.when(low >= 0)
        def _():
            g_copy(c, low, 0).wait_recv()
            pl.when(not_top)(lambda: g_copy(c, low, 0).start())

    def g_high(c, s):
        high = z + 1 + s

        @pl.when(high <= L - 1)
        def _():
            g_copy(c, high, 1).wait_recv()
            pl.when(not_bottom)(lambda: g_copy(c, high, 1).start())

    def g_slot(c, s):
        g_low(c, s)
        g_high(c, s)

    def g_lead(c):
        for ahead in range(1, L - 2):
            for k in range(ahead):
                for s in range(L - 2 - ahead):
                    pl.when(z == L - 2 - ahead)(lambda: g_low(c + k, s))
                    pl.when(z == 1 + ahead)(lambda: g_high(c + k, s))

    def g_slot_ahead(c, s):
        for ahead in range(L - 2):
            fits = c + ahead < n
            pl.when((z == L - 2 - ahead) & fits)(lambda: g_low(c + ahead, s))
            pl.when((z == 1 + ahead) & fits)(lambda: g_high(c + ahead, s))
        pl.when(z == L - 1)(lambda: g_low(c, s))
        pl.when(z == 0)(lambda: g_high(c, s))

    def block(c, b):
        return g.at[c, :, pl.ds(al(b * bd, bd), bd), :]

    def s_up(c, b):
        return remote(block(c, b), gin.at[c, b], sem_ss, sem_sr.at[c, b], dev_up)

    def s_down(c, b):
        return remote(block(c, b), gin.at[c, b], sem_ss, sem_sr.at[c, b], dev_down)

    def s_last_down(c, b):
        return remote(block(c, b), gin.at[c, L], sem_ss, sem_sr.at[c, L], dev_down)

    def add_in(c, b, *slots):
        for p in range(2):
            rows = pl.ds(al(b * bd, bd), bd)
            value = g[c, p, rows, :].astype(F32)
            for slot in slots:
                value = value + gin[c, slot, p].astype(F32)
            g[c, p, rows, :] = value.astype(BF)

    def s_slot_up(c, s):
        @pl.when((z <= s) & not_top)
        def _():
            b = L - 1 - s + z

            @pl.when(not_bottom)
            def _():
                s_up(c, b).wait_recv()
                add_in(c, b, b)

            s_up(c, b).start()

    def s_slot_down(c, s):
        @pl.when((L - 1 - z <= s) & not_bottom)
        def _():
            b = s - (L - 1) + z

            @pl.when(not_top)
            def _():
                s_down(c, b).wait_recv()
                add_in(c, b, b)

            if s == L - 2:
                s_last_down(c, b).start()
            else:
                s_down(c, b).start()

    def s_slot(c, s):
        s_slot_up(c, s)
        s_slot_down(c, s)

    def fin_side(c, p):
        return remote(
            g.at[c, p, pl.ds(al((z * 2 + 1 - y) * dp, dp), dp), :], gouts[p].at[:, w_cols(c, y)],
            sem_fy, sem_fyr, dev_y)

    def fin_local(c, p):
        return pltpu.make_async_copy(
            g.at[c, p, pl.ds(al((z * 2 + y) * dp, dp), dp), :], gouts[p].at[:, w_cols(c, y)], sem_fl)

    def finish(c):
        pl.when(not_bottom)(lambda: s_up(c, z).wait_recv())
        pl.when(not_top)(lambda: s_last_down(c, z).wait_recv())
        pl.when(z == 0)(lambda: add_in(c, z, L))
        pl.when(z == L - 1)(lambda: add_in(c, z, L - 1))
        pl.when(not_top & not_bottom)(lambda: add_in(c, z, z, L))
        for p in range(2):
            fin_side(c, p).start()
            fin_local(c, p).start()

    row_src = (saved_h, upst_h, fresh_h)
    row_dst = (rows_s, rows_u, rows_f)

    def spot(cc, xx, yy):
        return pl.ds(al(((cc * 2 + xx) * 2 + yy) * q, q), q)

    def row_local(a, j):
        return pltpu.make_async_copy(
            row_src[a].at[pl.ds(j * q, q), :], row_dst[a].at[spot(j % 2, j // 2, y), :], sem_rl.at[a])

    half_q = q // 2

    def spot_piece(cc, xx, yy, k):
        return pl.ds(al(((cc * 2 + xx) * 2 + yy) * q + k * half_q, half_q), half_q)

    def row_y(a, k):
        return remote(
            row_src[a].at[pl.ds(al(tp * q + k * half_q, half_q), half_q), :],
            row_dst[a].at[spot_piece(c0, x, y, k), :], sem_rys, sem_ryr.at[a, k], dev_y)

    def row_start(a):
        for k in range(2):
            row_y(a, k).start()

    def x_fwd(a, k):
        part = row_dst[a].at[spot_piece(c0, x, 1 - y, k), :]
        return remote(part, part, sem_rs.at[a], sem_rxr.at[a], dev_x)

    def d_fwd(a, k):
        part = row_dst[a].at[spot(c0, x if k == 0 else 1 - x, 1 - y), :]
        return remote(part, part, sem_rs.at[a], sem_rdr.at[a], dev_c)

    def rows_hop1(a, k):
        row_y(a, k).wait_recv()
        x_fwd(a, k).start()
        if k == 1:
            d_fwd(a, 0).start()

    def rows_hop2(a):
        all_sent(row_dst[a].at[spot(c0, 1 - x, 1 - y), :], sem_rxr.at[a])
        d_fwd(a, 1).start()

    def rows_sent(a):
        all_sent(row_dst[a].at[0:3 * q, :], sem_rs.at[a])

    def rows_ready(a):
        all_sent(row_dst[a].at[0:4 * q, :], sem_rl.at[a])
        all_sent(row_dst[a].at[0:2 * q, :], sem_rdr.at[a])

    def transpose(src, dst):
        tile = COL_TILE

        def step(i, carry):
            at = pl.ds(al(i * tile, tile), tile)
            dst[at, :] = src[:, at].T
            return carry

        lax.fori_loop(0, K // tile, step, 0)

    tm = min(ROW_TILE, Tk)

    def dot(a, b):
        return jnp.dot(a, b, preferred_element_type=F32)

    def saved_part(c):
        def step(t, carry):
            r = pl.ds(al(t * tm, tm), tm)
            active = jnp.maximum(dot(rows_s[r, :], w[c, 0]), 0.0)
            shid[r, :] = (active * active).astype(BF)
            pre[c, r, :] = (2.0 * active * dot(rows_u[r, :], w[c, 1])).astype(BF)
            return carry

        lax.fori_loop(0, Tk // tm, step, 0)

        def grad(b, carry):
            r = pl.ds(al(b * bd, bd), bd)
            g[c, 0, r, :] = dot(s_t[r, :], pre[c]).astype(BF)
            g[c, 1, r, :] = dot(u_t[r, :], shid[...]).astype(BF)
            return carry

        lax.fori_loop(0, L, grad, 0)
        s_slot(c, 0)
        pl.when(at_end)(lambda: end_slots(c))

    def fresh_part(c):
        def step(t, carry):
            r = pl.ds(al(t * tm, tm), tm)
            active = jnp.maximum(dot(rows_f[r, :], w[c, 0]), 0.0)
            hid[c, r, :] = (active * active).astype(BF)
            return carry

        lax.fori_loop(0, Tk // tm, step, 0)

    half_rows = Tk // 2

    pw = K // PIECES

    def out_piece(a, cc, h):
        left, stage, p = ((hid, rows_f, 1), (pre, rows_s, 0))[a]
        r = pl.ds(al(cc * half_rows, half_rows), half_rows)

        def step(d, carry):
            at = pl.ds(al(h * pw + d * COL_TILE, COL_TILE), COL_TILE)
            total = None
            for c in range(0, n, 2):
                term = against_rows(
                    jnp.concatenate((left[c, r, :], left[c + 1, r, :]), axis=1),
                    jnp.concatenate((w[c, p, at, :], w[c + 1, p, at, :]), axis=1))
                total = term if total is None else total + term
            stage[r, at] = total.astype(BF)
            return carry

        lax.fori_loop(0, pw // COL_TILE, step, 0)

    stages = (rows_f, rows_s)
    quarter = Tk // 4
    far_x = pl.ds(al(c0 * half_rows + (1 - x) * quarter, quarter), quarter)

    def cols(h):
        return pl.ds(h * pw, pw)

    def o1(a, h):
        return remote(
            stages[a].at[pl.ds(al((1 - c0) * half_rows, half_rows), half_rows), cols(h)], r1.at[a, :, cols(h)],
            sem_os.at[a, 0], sem_or.at[a, 0, h], dev_c)

    def o2(a, h):
        return remote(
            stages[a].at[far_x, cols(h)], r2.at[a, :, cols(h)], sem_os.at[a, 1], sem_or.at[a, 1, h], dev_x)

    def o3(a, h):
        return remote(
            stages[a].at[spot(c0, x, 1 - y), cols(h)], r3.at[a, :, cols(h)],
            sem_os.at[a, 2], sem_or.at[a, 2, h], dev_y)

    def join(a, at, h, *terms):
        value = stages[a][at, cols(h)].astype(F32)
        for t in terms:
            value = value + t.astype(F32)
        return value

    def out_c(a, h):
        out_piece(a, 1 - c0, h)
        o1(a, h).start()

    def out_x(a, h):
        out_piece(a, c0, h)
        o1(a, h).wait_recv()
        part = r1[a, pl.ds(al((1 - x) * quarter, quarter), quarter), cols(h)]
        stages[a][far_x, cols(h)] = join(a, far_x, h, part).astype(BF)
        o2(a, h).start()

    def out_pair(a, h):
        out_c(a, h)
        out_c(a, h + 1)
        out_x(a, h)
        out_x(a, h + 1)

    def pieces(a, yy, h):
        return (r1[a, pl.ds(al(x * quarter + yy * q, q), q), cols(h)],
                r2[a, pl.ds(al(yy * q, q), q), cols(h)])

    def out_y(a, h):
        o2(a, h).wait_recv()
        at = spot(c0, x, 1 - y)
        stages[a][at, cols(h)] = join(a, at, h, *pieces(a, 1 - y, h)).astype(BF)
        o3(a, h).start()

    def out_local(a, h):
        return pltpu.make_async_copy(
            stages[a].at[spot(c0, x, y), cols(h)], (fo, so)[a].at[:, cols(h)], sem_ol.at[a])

    def out_end(a, h):
        o3(a, h).wait_recv()
        at = spot(c0, x, y)
        stages[a][at, cols(h)] = join(a, at, h, *pieces(a, y, h), r3[a, :, cols(h)]).astype(BF)
        out_local(a, h).start()

    def end_slots(c):
        for s in range(1, L - 2):
            s_slot(c, s)

    def mid_slots(c):
        pl.when(jnp.logical_not(at_end))(lambda: end_slots(c))

    def over(low, high, fn):
        if high > low:
            lax.fori_loop(low, high, lambda c, carry: (fn(c), carry)[1], 0)

    middle = range(1, L - 2)
    for c in range(2):
        w_start_local(c)
    pl.when(not_top)(lambda: greet(dev_up))
    pl.when(not_bottom)(lambda: greet(dev_down))
    greet(dev_y)
    greet(dev_x)
    greet(dev_c)
    over(2, n, w_start_local)
    for a in range(3):
        for j in range(4):
            row_local(a, j).start()
    pl.semaphore_wait(barrier, 3 + jnp.where(not_top, 1, 0) + jnp.where(not_bottom, 1, 0))
    start_w(0)
    start_w(1)
    row_y(0, 0).start()
    start_w(2)
    row_y(0, 1).start()
    start_w(3)
    row_y(1, 0).start()
    row_y(1, 1).start()
    over(4, n, start_w)
    row_y(2, 0).start()
    row_y(2, 1).start()

    g_local(0, 2)
    for c in range(2):
        for lead in range(3):
            g_near(lead, c)
    g_local(2, n)
    g_side(0)
    for lead in range(3):
        g_far(lead, 0)
    g_near(2, 2)
    g_side(1)
    g_far(2, 1)
    g_far(0, 1)
    g_near(2, 3)
    g_near(2, 4)
    g_slot(0, 0)
    g_near(0, 2)
    g_far(1, 1)
    rows_hop1(0, 0)
    g_side(2)
    g_far(2, 2)
    g_near(2, 5)
    g_near(2, 6)
    for s in middle:
        g_slot(0, s)
    rows_hop1(0, 1)
    g_slot(0, L - 2)
    g_own(1, 2)
    g_slot(1, 0)
    g_far(0, 2)
    g_side(3)
    g_far(2, 3)
    over(7, n, lambda c: g_near(2, c))
    rows_hop2(0)
    g_own(1, 3)
    rows_hop1(1, 0)
    rows_ready(0)
    transpose(rows_s, s_t)
    for s in middle:
        g_slot(1, s)
    rows_hop1(1, 1)
    g_side(4)
    g_far(2, 4)
    g_own(1, 4)
    rows_hop2(1)
    g_slot(1, L - 2)
    g_side(5)
    g_far(2, 5)
    rows_ready(1)
    transpose(rows_u, u_t)
    g_lead(2)
    g_slot_ahead(2, 0)
    g_own(0, 3)
    g_own(1, 5)
    over(6, n - 1, g_side)
    over(6, n - 1, lambda c: g_far(2, c))
    saved_part(0)
    g_side(n - 1)
    g_far(2, n - 1)
    g_own(1, 6)
    for s in middle:
        g_slot_ahead(2, s)
    saved_part(1)
    g_slot_ahead(2, L - 2)
    rows_hop1(2, 0)
    rows_hop1(2, 1)
    g_slot_ahead(3, 0)
    g_own(0, 4)
    over(7, n, lambda c: g_own(1, c))
    for s in middle:
        g_slot_ahead(3, s)
    s_last(2, 0)
    saved_part(2)
    mid_slots(0)
    rows_hop2(2)
    g_slot_ahead(3, L - 2)
    rows_ready(2)
    over(0, 3, fresh_part)
    mid_slots(1)

    def period(c):
        g_slot_ahead(c, 0)
        pl.when(c + 1 < n)(lambda: g_own(0, c + 1))
        for s in middle:
            g_slot_ahead(c, s)
        saved_part(c - 1)
        fresh_part(c - 1)
        mid_slots(c - 2)
        pl.when(c < n - 1)(lambda: s_last(2, c - 3))
        pl.when(c >= 5)(lambda: s_last(1, c - 5))
        g_slot_ahead(c, L - 2)

    over(4, n, period)

    def at_ends(c):
        pl.when(at_end)(lambda: finish(c))

    def inside(c):
        pl.when(jnp.logical_not(at_end))(lambda: finish(c))

    over(0, n - 3, lambda c: s_last(0, c))
    s_last(1, n - 5)
    s_last(1, n - 4)
    fresh_part(n - 1)
    for a in (0, 2):
        rows_sent(a)
    out_c(0, 0)
    out_c(0, 1)
    out_x(0, 0)
    out_x(0, 1)
    at_ends(0)
    inside(0)
    inside(1)
    mid_slots(n - 2)
    s_last(0, n - 3)
    s_last(1, n - 3)
    saved_part(n - 1)
    over(n - 4, n, lambda c: s_last(2, c))
    at_ends(1)
    inside(2)
    out_y(0, 0)
    out_c(0, 2)
    out_c(0, 3)
    out_x(0, 2)
    out_x(0, 3)
    out_y(0, 1)
    at_ends(2)
    out_c(1, 0)
    out_c(1, 1)
    out_x(1, 0)
    mid_slots(n - 1)
    s_last(0, n - 2)
    s_last(1, n - 2)
    out_x(1, 1)
    finish(3)
    out_y(0, 2)
    out_c(1, 2)
    out_c(1, 3)
    out_x(1, 2)
    out_x(1, 3)
    s_last(1, n - 1)
    out_y(0, 3)
    over(4, n - 3, finish)
    s_last(0, n - 1)
    out_y(1, 0)
    finish(n - 3)
    out_y(1, 1)
    at_ends(n - 2)
    out_y(1, 2)
    inside(n - 2)
    at_ends(n - 1)
    out_y(1, 3)
    inside(n - 1)
    for h in range(PIECES):
        out_end(0, h)
    for h in range(PIECES):
        out_end(1, h)

    all_sent(w.at[:, :, 0:dp, :], sem_wys)
    for k in range(L):
        pl.when((z == k) & not_top)(lambda: all_sent(w.at[:, :, 0:(k + 1) * bd, :], sem_gs.at[0]))
        pl.when((z == k) & not_bottom)(lambda: all_sent(w.at[:, :, 0:(L - k) * bd, :], sem_gs.at[1]))
    all_sent(g.at[:, :, 0:(L - 1) * bd, :], sem_ss)
    for sem in (sem_fy, sem_fyr, sem_fl):
        all_sent(g.at[:, :, 0:dp, :], sem)
    all_sent(rows_s.at[0:3 * q, :], sem_rys)
    rows_sent(1)
    for a in range(2):
        for k, count in enumerate((half_rows, quarter, q)):
            all_sent(stages[a].at[0:count, :], sem_os.at[a, k])
        all_sent(stages[a].at[0:q, :], sem_ol.at[a])


def finish_kernel(grad_scale, fresh_in, saved_in, up_in, down_in, up_sum, down_sum, fresh, saved, up, down):
    fresh[...] = fresh_in[...]
    saved[...] = saved_in[...]
    up[...] = up_in[...] + grad_scale * up_sum[...].astype(F32)
    down[...] = down_in[...] + grad_scale * down_sum[...].astype(F32)


def finish_call(grad_scale, *arrays):
    steps = 2

    def spec(a):
        return pl.BlockSpec((a.shape[0] // steps, a.shape[1]), lambda i: (i, 0))

    outs = arrays[:4]
    return pl.pallas_call(
        functools.partial(finish_kernel, grad_scale),
        grid=(steps,),
        in_specs=[spec(a) for a in arrays],
        out_specs=[spec(a) for a in outs],
        out_shape=[jax.ShapeDtypeStruct(a.shape, a.dtype) for a in outs],
        cost_estimate=pl.CostEstimate(flops=2**20, bytes_accessed=2**24, transcendentals=0),
    )(*arrays)


def fused_body(plan, fresh_rows, saved_rows, upstream_grad, proj_up, proj_down, accum_up, accum_down):
    L, q, dp, K, H, n, cw, Tk = (plan[k] for k in ("L", "q", "dp", "K", "H", "n", "w", "Tk"))
    fs_n = lax.axis_size("fs")
    grad_scale = float(fresh_rows.shape[0] * fs_n) ** (-0.5)
    dma = lambda *shape: pltpu.SemaphoreType.DMA(shape)
    one = pltpu.SemaphoreType.DMA
    vm = lambda *shape: pltpu.VMEM(shape, BF)
    flops = 2 * 6 * Tk * K * H
    any_spec = pl.BlockSpec(memory_space=pl.ANY)
    fresh_out, saved_grad, up_sum, down_sum = pl.pallas_call(
        functools.partial(layer_kernel, plan),
        out_shape=(
            jax.ShapeDtypeStruct((q, K), BF),
            jax.ShapeDtypeStruct((q, K), BF),
            jax.ShapeDtypeStruct((dp, 2 * H), BF),
            jax.ShapeDtypeStruct((dp, 2 * H), BF),
        ),
        in_specs=[any_spec] * 5,
        out_specs=(any_spec,) * 4,
        scratch_shapes=[
            vm(Tk, K), vm(Tk, K), vm(Tk, K), vm(K, Tk), vm(K, Tk),
            vm(n, 2, K, cw), vm(n, Tk, cw), vm(n, Tk, cw), vm(Tk, cw),
            vm(n, 2, K, cw), vm(n, L + 1, 2, 2 * dp, cw),
            vm(2, Tk // 2, K), vm(2, Tk // 4, K), vm(2, q, K),
            dma(2), one, dma(n), dma(2), dma(n, L), one, dma(n, L + 1), one, one, one,
            dma(3), one, dma(3, 2), dma(3), dma(3), dma(3), dma(2, 3), dma(2, 3, PIECES), dma(2),
        ],
        compiler_params=pltpu.CompilerParams(
            collective_id=0, has_side_effects=True, vmem_limit_bytes=67043328),
        cost_estimate=pl.CostEstimate(flops=flops, bytes_accessed=2**24, transcendentals=0),
    )(fresh_rows, saved_rows, upstream_grad, proj_up, proj_down)
    return finish_call(grad_scale, fresh_out, saved_grad, accum_up, accum_down, up_sum, down_sum)


def any_body(*args):
    plan = make_plan(
        lax.axis_size("fs"), lax.axis_size("tp"), args[0].shape[0], args[0].shape[1],
        args[3].shape[0], args[3].shape[1], CHUNKS)
    if plan is None:
        return body(*args)
    return fused_body(plan, *args)


def solution(mesh):
    in_specs = (P("fs", None),) * 3 + (P("fs", "tp"),) * 4
    out_specs = (P(("fs", "tp"), None),) * 2 + (P("fs", "tp"),) * 2
    return jax.shard_map(any_body, mesh=mesh, in_specs=in_specs, out_specs=out_specs, check_vma=False)
```

```python
import functools

import jax
import jax.numpy as jnp
from jax import lax
from jax.experimental import pallas as pl
from jax.experimental.pallas import tpu as pltpu
from jax.sharding import PartitionSpec as P


BF = jnp.bfloat16
F32 = jnp.float32


def against_rows(left, right):
    return lax.dot_general(left, right, (((1,), (1,)), ((), ())), preferred_element_type=F32)


def over_tokens(left, right):
    return lax.dot_general(left, right, (((0,), (0,)), ((), ())), preferred_element_type=F32)


def squared_relu(pre_values):
    active = jnp.maximum(pre_values, 0.0)
    return (active, (active * active).astype(BF))


def after(value, *earlier):
    return lax.optimization_barrier((value, earlier))[0]


def body(fresh_rows, saved_rows, upstream_grad, proj_up, proj_down, accum_up, accum_down):
    fs_n, tp_n = lax.axis_size("fs"), lax.axis_size("tp")
    line_n = fs_n // 2
    fs, tp = lax.axis_index("fs"), lax.axis_index("tp")
    line, side = fs // 2, fs % 2
    row_count, width = fresh_rows.shape
    depth, columns = proj_up.shape
    half = columns // 2
    grad_scale = float(row_count * fs_n) ** (-0.5)

    def to_side(value):
        return lax.ppermute(value, "fs", [(i, i ^ 1) for i in range(fs_n)])

    def to_tp(value, bit):
        return lax.ppermute(value, "tp", [(j, j ^ bit) for j in range(tp_n)])

    def along(value, lines, way):
        return lax.ppermute(
            value,
            "fs",
            [(l * 2 + s, (l + way) * 2 + s) for l in lines for s in range(2)],
        )

    def side_block(weight):
        mine = lax.dynamic_slice_in_dim(weight, side * half, half, 1)
        other = lax.dynamic_slice_in_dim(weight, (1 - side) * half, half, 1)
        return mine, to_side(other)

    def line_gather(block, ties={}):
        ups, downs = [block], [block]
        for step in range(1, line_n):
            up, down = after((ups[-1], downs[-1]), *ties.get(step, ()))
            up = along(up, range(step - 1, line_n - 1), 1)
            down = along(down, range(1, line_n - step + 1), -1)
            up, down = lax.optimization_barrier((up, down))
            ups.append(up)
            downs.append(down)
        blocks = [block] + [
            jnp.where(line >= k, ups[k], downs[line_n - k]) for k in range(1, line_n)
        ]
        return jnp.concatenate(blocks, axis=0), ups

    def line_sum(grads, ties={}):
        size = 2 * depth
        up = down = None
        marks = []
        for step in range(1, line_n):
            low = grads[step * size : (step + 1) * size]
            high = grads[(line_n - step) * size : (line_n - step + 1) * size]
            low = low if up is None else low + up.astype(F32)
            high = high if down is None else high + down.astype(F32)
            low, high = after((low.astype(BF), high.astype(BF)), *ties.get(step, ()))
            up = along(low, range(0, step), 1)
            down = along(high, range(line_n - step, line_n), -1)
            up, down = lax.optimization_barrier((up, down))
            marks.append(up)
        return grads[:size] + up.astype(F32) + down.astype(F32), marks

    def finish_grad(accum, total, other):
        mine = total[:depth]
        other = other.astype(F32)
        return accum + jnp.where(
            side == 0,
            jnp.concatenate((mine, other), axis=1),
            jnp.concatenate((other, mine), axis=1),
        )

    order = [lax.rem(line - k + line_n, line_n) * 2 + (side ^ j) for k in range(line_n) for j in range(2)]
    core = tp % 2

    def near_rows(rows):
        piece = row_count // 2
        return to_side(lax.dynamic_slice_in_dim(rows, core * piece, piece, 0))

    def both_sides(rows, near):
        far = to_tp(near, 1)
        rows = jnp.concatenate(
            (rows, jnp.where(core == 0, near, far), jnp.where(core == 0, far, near)), axis=0
        )
        return jnp.concatenate(
            [lax.dynamic_slice_in_dim(rows, o * depth, depth, 1) for o in order], axis=1
        )

    def share_tp(term):
        value = term.astype(BF)
        bit, stages = 1, []
        outer = 2 * tp_n
        rest = row_count // tp_n
        value = value.reshape(2 * tp_n, rest, width)
        while bit < tp_n:
            outer //= 2
            view = value.reshape(outer, 2, rest, width)
            mine = (tp // bit) % 2
            keep = lax.dynamic_index_in_dim(view, mine, 1, keepdims=False)
            send = lax.dynamic_index_in_dim(view, 1 - mine, 1, keepdims=False)
            value = (keep.astype(F32) + to_tp(send, bit).astype(F32)).astype(BF)
            bit *= 2
            stages.append(value)
        return stages

    def share_side(value):
        blocks = [
            lax.dynamic_slice_in_dim(
                value, (lax.rem(line - b // 2 + line_n, line_n) * 2 + (side ^ (b % 2))) * depth, depth, 2
            )
            for b in range(fs_n)
        ]
        value = jnp.concatenate(blocks, axis=2)
        return (value[0].astype(F32) + to_side(value[1]).astype(F32)).astype(BF)

    up_pair = side_block(proj_up)
    down_pair = side_block(proj_down)
    rows = after((saved_rows, upstream_grad, fresh_rows), down_pair[1])
    nears = [near_rows(r) for r in rows]
    up_whole, ups = line_gather(jnp.concatenate(up_pair, axis=0))
    saved_all = both_sides(rows[0], after(nears[0], ups[max(line_n - 2, 1)]))
    upstream_all = both_sides(rows[1], after(nears[1], ups[-1]))
    down_start = after(jnp.concatenate(down_pair, axis=0), ups[-1])
    saved_pre = jnp.dot(saved_all, up_whole, preferred_element_type=F32)
    saved_active, saved_hidden = squared_relu(saved_pre)
    down_grads = grad_scale * over_tokens(upstream_all, saved_hidden)
    down_total, _ = line_sum(down_grads)
    fresh_all = both_sides(rows[2], after(nears[2], down_grads))
    fresh_hidden = squared_relu(jnp.dot(fresh_all, up_whole, preferred_element_type=F32))[1]
    down_whole, _ = line_gather(down_start, {2: (down_grads,), 3: (fresh_hidden,)})
    hidden_grad = jnp.dot(upstream_all, down_whole, preferred_element_type=F32)
    pre_grad = (2.0 * saved_active * hidden_grad).astype(BF)
    up_grads = grad_scale * over_tokens(saved_all, pre_grad)
    fresh_hidden, pre_grad, _ = lax.optimization_barrier((fresh_hidden, pre_grad, up_grads))
    fresh_stages = share_tp(against_rows(fresh_hidden, down_whole))
    saved_stages = share_tp(against_rows(pre_grad, up_whole))
    up_total, marks = line_sum(
        up_grads, {2: (fresh_stages[0], saved_stages[0]), 3: (fresh_stages[-1],)}
    )
    middle = marks[max(line_n - 3, 0)]
    fresh_out = share_side(fresh_stages[-1])
    saved_grad = share_side(saved_stages[-1])
    down_other = after(to_side(down_total[depth:].astype(BF)), middle)
    accum_down_out = finish_grad(accum_down, down_total, down_other)
    accum_up_out = finish_grad(accum_up, up_total, to_side(up_total[depth:].astype(BF)))
    return (fresh_out, saved_grad, accum_up_out, accum_down_out)


MESH = pl.DeviceIdType.MESH
CHUNKS = 8
ROW_TILE = 512
COL_TILE = 256
PIECES = 4


def make_plan(fs_n, tp_n, row_count, width, depth, columns, chunks):
    half = columns // 2
    if tp_n != 4 or fs_n % 2 or fs_n < 6 or half % chunks or (half // chunks) % 128 or chunks < 8 or chunks % 2 or fs_n < 8:
        return None
    if row_count % 128 or depth % 16 or width % (COL_TILE * PIECES):
        return None
    lines, tokens = fs_n // 2, 2 * row_count
    words = 5 * tokens * width + 2 * 2 * width * half + 2 * tokens * half + tokens * half // chunks
    words += 2 * (lines + 1) * 2 * depth * half + 2 * (tokens // 2 + tokens // 4 + tokens // 8) * width
    words += 2 * (tokens // 8) * width
    if 2 * words > 60 * 2**20:
        return None
    return dict(L=lines, q=row_count // 4, dp=depth, K=width, H=half, n=chunks, w=half // chunks, Tk=tokens)


def layer_kernel(plan, fresh_h, saved_h, upst_h, wu_h, wd_h, fo, so, gup, gdown,
                 rows_s, rows_u, rows_f, s_t, u_t, w, hid, pre, shid, g, gin, r1, r2, r3,
                 sem_wl, sem_wys, sem_wyr, sem_gs, sem_gr, sem_ss, sem_sr, sem_fy, sem_fyr, sem_fl,
                 sem_rl, sem_rys, sem_ryr, sem_rs, sem_rxr, sem_rdr, sem_os, sem_or, sem_ol):
    L, q, dp, K, H, n, cw, Tk = (plan[k] for k in ("L", "q", "dp", "K", "H", "n", "w", "Tk"))
    bd = 2 * dp
    gouts = (gup, gdown)
    fs, tp = lax.axis_index("fs"), lax.axis_index("tp")
    z, y = fs // 2, fs % 2
    x, c0 = tp // 2, tp % 2
    not_top, not_bottom = z < L - 1, z > 0
    dev_up, dev_down = (fs + 2, tp), (fs - 2, tp)
    dev_y = (z * 2 + (1 - y), tp)
    dev_x = (fs, (1 - x) * 2 + c0)
    dev_c = (fs, x * 2 + (1 - c0))

    def remote(src, dst, send, recv, dev):
        return pltpu.make_async_remote_copy(
            src_ref=src, dst_ref=dst, send_sem=send, recv_sem=recv, device_id=dev, device_id_type=MESH)

    def all_sent(ref, sem):
        pltpu.make_async_copy(ref, ref, sem).wait()

    def al(value, size):
        return pl.multiple_of(value, size)

    barrier = pltpu.get_barrier_semaphore()

    def greet(dev):
        pl.semaphore_signal(barrier, inc=1, device_id=dev, device_id_type=MESH)

    def w_cols(c, side):
        return pl.ds(al(side * H + c * cw, 128), cw)

    w_src = (wu_h, wd_h)
    my_rows = pl.ds(al((z * 2 + y) * dp, dp), dp)
    side_rows = pl.ds(al((z * 2 + 1 - y) * dp, dp), dp)

    def w_local(c, p):
        return pltpu.make_async_copy(
            w_src[p].at[:, w_cols(c, y)], w.at[c, p, my_rows, :], sem_wl.at[jnp.where(c < 2, 0, 1)])

    def w_side(c, p):
        return remote(
            w_src[p].at[:, w_cols(c, 1 - y)], w.at[c, p, my_rows, :], sem_wys, sem_wyr.at[c], dev_y)

    def start_w(c):
        for p in range(2):
            w_side(c, p).start()

    def w_start_local(c):
        for p in range(2):
            w_local(c, p).start()

    def g_copy(c, b, way):
        part = w.at[c, :, pl.ds(al(b * bd, bd), bd), :]
        return remote(part, part, sem_gs.at[way], sem_gr.at[c, b], (dev_up, dev_down)[way])

    def g_local(low, high):
        all_sent(w.at[low:high, :, my_rows, :], sem_wl.at[0 if low == 0 else 1])

    def g_side(c):
        all_sent(w.at[c, :, side_rows, :], sem_wyr.at[c])

    def by_lead(lead, up, down):
        leads = range(lead, L - 1) if lead == 2 else (lead,)
        for a in leads:
            pl.when(z == L - 2 - a)(up)
            pl.when(z == 1 + a)(down)

    def g_part(c, side, way):
        rows = w.at[c, :, pl.ds(al((z * 2 + side) * dp, dp), dp), :]
        remote(rows, rows, sem_gs.at[way], sem_gr.at[c, z], (dev_up, dev_down)[way]).start()

    def g_near(lead, c):
        by_lead(lead, lambda: g_part(c, y, 0), lambda: g_part(c, y, 1))

    def g_far(lead, c):
        by_lead(lead, lambda: g_part(c, 1 - y, 0), lambda: g_part(c, 1 - y, 1))

    def g_own(lead, c):
        g_near(lead, c)
        g_far(lead, c)

    def s_last(lead, c):
        by_lead(lead, lambda: s_slot_up(c, L - 2), lambda: s_slot_down(c, L - 2))

    at_end = (z == 0) | (z == L - 1)

    def g_low(c, s):
        low = z - 1 - s

        @pl.when(low >= 0)
        def _():
            g_copy(c, low, 0).wait_recv()
            pl.when(not_top)(lambda: g_copy(c, low, 0).start())

    def g_high(c, s):
        high = z + 1 + s

        @pl.when(high <= L - 1)
        def _():
            g_copy(c, high, 1).wait_recv()
            pl.when(not_bottom)(lambda: g_copy(c, high, 1).start())

    def g_slot(c, s):
        g_low(c, s)
        g_high(c, s)

    def g_lead(c):
        for ahead in range(1, L - 2):
            for k in range(ahead):
                for s in range(L - 2 - ahead):
                    pl.when(z == L - 2 - ahead)(lambda: g_low(c + k, s))
                    pl.when(z == 1 + ahead)(lambda: g_high(c + k, s))

    def g_slot_ahead(c, s):
        for ahead in range(L - 2):
            fits = c + ahead < n
            pl.when((z == L - 2 - ahead) & fits)(lambda: g_low(c + ahead, s))
            pl.when((z == 1 + ahead) & fits)(lambda: g_high(c + ahead, s))
        pl.when(z == L - 1)(lambda: g_low(c, s))
        pl.when(z == 0)(lambda: g_high(c, s))

    def block(c, b):
        return g.at[c, :, pl.ds(al(b * bd, bd), bd), :]

    def s_up(c, b):
        return remote(block(c, b), gin.at[c, b], sem_ss, sem_sr.at[c, b], dev_up)

    def s_down(c, b):
        return remote(block(c, b), gin.at[c, b], sem_ss, sem_sr.at[c, b], dev_down)

    def s_last_down(c, b):
        return remote(block(c, b), gin.at[c, L], sem_ss, sem_sr.at[c, L], dev_down)

    def add_in(c, b, *slots):
        for p in range(2):
            rows = pl.ds(al(b * bd, bd), bd)
            value = g[c, p, rows, :].astype(F32)
            for slot in slots:
                value = value + gin[c, slot, p].astype(F32)
            g[c, p, rows, :] = value.astype(BF)

    def s_slot_up(c, s):
        @pl.when((z <= s) & not_top)
        def _():
            b = L - 1 - s + z

            @pl.when(not_bottom)
            def _():
                s_up(c, b).wait_recv()
                add_in(c, b, b)

            s_up(c, b).start()

    def s_slot_down(c, s):
        @pl.when((L - 1 - z <= s) & not_bottom)
        def _():
            b = s - (L - 1) + z

            @pl.when(not_top)
            def _():
                s_down(c, b).wait_recv()
                add_in(c, b, b)

            if s == L - 2:
                s_last_down(c, b).start()
            else:
                s_down(c, b).start()

    def s_slot(c, s):
        s_slot_up(c, s)
        s_slot_down(c, s)

    def fin_side(c, p):
        return remote(
            g.at[c, p, pl.ds(al((z * 2 + 1 - y) * dp, dp), dp), :], gouts[p].at[:, w_cols(c, y)],
            sem_fy, sem_fyr, dev_y)

    def fin_local(c, p):
        return pltpu.make_async_copy(
            g.at[c, p, pl.ds(al((z * 2 + y) * dp, dp), dp), :], gouts[p].at[:, w_cols(c, y)], sem_fl)

    def finish(c):
        pl.when(not_bottom)(lambda: s_up(c, z).wait_recv())
        pl.when(not_top)(lambda: s_last_down(c, z).wait_recv())
        pl.when(z == 0)(lambda: add_in(c, z, L))
        pl.when(z == L - 1)(lambda: add_in(c, z, L - 1))
        pl.when(not_top & not_bottom)(lambda: add_in(c, z, z, L))
        for p in range(2):
            fin_side(c, p).start()
            fin_local(c, p).start()

    row_src = (saved_h, upst_h, fresh_h)
    row_dst = (rows_s, rows_u, rows_f)

    def spot(cc, xx, yy):
        return pl.ds(al(((cc * 2 + xx) * 2 + yy) * q, q), q)

    def row_local(a, j):
        return pltpu.make_async_copy(
            row_src[a].at[pl.ds(j * q, q), :], row_dst[a].at[spot(j % 2, j // 2, y), :], sem_rl.at[a])

    half_q = q // 2

    def spot_piece(cc, xx, yy, k):
        return pl.ds(al(((cc * 2 + xx) * 2 + yy) * q + k * half_q, half_q), half_q)

    def row_y(a, k):
        return remote(
            row_src[a].at[pl.ds(al(tp * q + k * half_q, half_q), half_q), :],
            row_dst[a].at[spot_piece(c0, x, y, k), :], sem_rys, sem_ryr.at[a, k], dev_y)

    def row_start(a):
        for k in range(2):
            row_y(a, k).start()

    def x_fwd(a, k):
        part = row_dst[a].at[spot_piece(c0, x, 1 - y, k), :]
        return remote(part, part, sem_rs.at[a], sem_rxr.at[a], dev_x)

    def d_fwd(a, k):
        part = row_dst[a].at[spot(c0, x if k == 0 else 1 - x, 1 - y), :]
        return remote(part, part, sem_rs.at[a], sem_rdr.at[a], dev_c)

    def rows_hop1(a, k):
        row_y(a, k).wait_recv()
        x_fwd(a, k).start()
        if k == 1:
            d_fwd(a, 0).start()

    def rows_hop2(a):
        all_sent(row_dst[a].at[spot(c0, 1 - x, 1 - y), :], sem_rxr.at[a])
        d_fwd(a, 1).start()

    def rows_sent(a):
        all_sent(row_dst[a].at[0:3 * q, :], sem_rs.at[a])

    def rows_ready(a):
        all_sent(row_dst[a].at[0:4 * q, :], sem_rl.at[a])
        all_sent(row_dst[a].at[0:2 * q, :], sem_rdr.at[a])

    def transpose(src, dst):
        tile = COL_TILE

        def step(i, carry):
            at = pl.ds(al(i * tile, tile), tile)
            dst[at, :] = src[:, at].T
            return carry

        lax.fori_loop(0, K // tile, step, 0)

    tm = min(ROW_TILE, Tk)

    def dot(a, b):
        return jnp.dot(a, b, preferred_element_type=F32)

    def saved_part(c):
        def step(t, carry):
            r = pl.ds(al(t * tm, tm), tm)
            active = jnp.maximum(dot(rows_s[r, :], w[c, 0]), 0.0)
            shid[r, :] = (active * active).astype(BF)
            pre[c, r, :] = (2.0 * active * dot(rows_u[r, :], w[c, 1])).astype(BF)
            return carry

        lax.fori_loop(0, Tk // tm, step, 0)

        def grad(b, carry):
            r = pl.ds(al(b * bd, bd), bd)
            g[c, 0, r, :] = dot(s_t[r, :], pre[c]).astype(BF)
            g[c, 1, r, :] = dot(u_t[r, :], shid[...]).astype(BF)
            return carry

        lax.fori_loop(0, L, grad, 0)
        s_slot(c, 0)
        pl.when(at_end)(lambda: end_slots(c))

    def fresh_part(c):
        def step(t, carry):
            r = pl.ds(al(t * tm, tm), tm)
            active = jnp.maximum(dot(rows_f[r, :], w[c, 0]), 0.0)
            hid[c, r, :] = (active * active).astype(BF)
            return carry

        lax.fori_loop(0, Tk // tm, step, 0)

    half_rows = Tk // 2

    pw = K // PIECES

    def out_piece(a, cc, h):
        left, stage, p = ((hid, rows_f, 1), (pre, rows_s, 0))[a]
        r = pl.ds(al(cc * half_rows, half_rows), half_rows)

        def step(d, carry):
            at = pl.ds(al(h * pw + d * COL_TILE, COL_TILE), COL_TILE)
            total = None
            for c in range(0, n, 2):
                term = against_rows(
                    jnp.concatenate((left[c, r, :], left[c + 1, r, :]), axis=1),
                    jnp.concatenate((w[c, p, at, :], w[c + 1, p, at, :]), axis=1))
                total = term if total is None else total + term
            stage[r, at] = total.astype(BF)
            return carry

        lax.fori_loop(0, pw // COL_TILE, step, 0)

    stages = (rows_f, rows_s)
    quarter = Tk // 4
    far_x = pl.ds(al(c0 * half_rows + (1 - x) * quarter, quarter), quarter)

    def cols(h):
        return pl.ds(h * pw, pw)

    def o1(a, h):
        return remote(
            stages[a].at[pl.ds(al((1 - c0) * half_rows, half_rows), half_rows), cols(h)], r1.at[a, :, cols(h)],
            sem_os.at[a, 0], sem_or.at[a, 0, h], dev_c)

    def o2(a, h):
        return remote(
            stages[a].at[far_x, cols(h)], r2.at[a, :, cols(h)], sem_os.at[a, 1], sem_or.at[a, 1, h], dev_x)

    def o3(a, h):
        return remote(
            stages[a].at[spot(c0, x, 1 - y), cols(h)], r3.at[a, :, cols(h)],
            sem_os.at[a, 2], sem_or.at[a, 2, h], dev_y)

    def join(a, at, h, *terms):
        value = stages[a][at, cols(h)].astype(F32)
        for t in terms:
            value = value + t.astype(F32)
        return value

    def out_c(a, h):
        out_piece(a, 1 - c0, h)
        o1(a, h).start()

    def out_x(a, h):
        out_piece(a, c0, h)
        o1(a, h).wait_recv()
        part = r1[a, pl.ds(al((1 - x) * quarter, quarter), quarter), cols(h)]
        stages[a][far_x, cols(h)] = join(a, far_x, h, part).astype(BF)
        o2(a, h).start()

    def out_pair(a, h):
        out_c(a, h)
        out_c(a, h + 1)
        out_x(a, h)
        out_x(a, h + 1)

    def pieces(a, yy, h):
        return (r1[a, pl.ds(al(x * quarter + yy * q, q), q), cols(h)],
                r2[a, pl.ds(al(yy * q, q), q), cols(h)])

    def out_y(a, h):
        o2(a, h).wait_recv()
        at = spot(c0, x, 1 - y)
        stages[a][at, cols(h)] = join(a, at, h, *pieces(a, 1 - y, h)).astype(BF)
        o3(a, h).start()

    def out_local(a, h):
        return pltpu.make_async_copy(
            stages[a].at[spot(c0, x, y), cols(h)], (fo, so)[a].at[:, cols(h)], sem_ol.at[a])

    def out_end(a, h):
        o3(a, h).wait_recv()
        at = spot(c0, x, y)
        stages[a][at, cols(h)] = join(a, at, h, *pieces(a, y, h), r3[a, :, cols(h)]).astype(BF)
        out_local(a, h).start()

    def end_slots(c):
        for s in range(1, L - 2):
            s_slot(c, s)

    def mid_slots(c):
        pl.when(jnp.logical_not(at_end))(lambda: end_slots(c))

    def over(low, high, fn):
        if high > low:
            lax.fori_loop(low, high, lambda c, carry: (fn(c), carry)[1], 0)

    middle = range(1, L - 2)
    for c in range(2):
        w_start_local(c)
    pl.when(not_top)(lambda: greet(dev_up))
    pl.when(not_bottom)(lambda: greet(dev_down))
    greet(dev_y)
    greet(dev_x)
    greet(dev_c)
    over(2, n, w_start_local)
    for a in range(3):
        for j in range(4):
            row_local(a, j).start()
    pl.semaphore_wait(barrier, 3 + jnp.where(not_top, 1, 0) + jnp.where(not_bottom, 1, 0))
    start_w(0)
    start_w(1)
    row_y(0, 0).start()
    start_w(2)
    row_y(0, 1).start()
    start_w(3)
    row_y(1, 0).start()
    row_y(1, 1).start()
    over(4, n, start_w)
    row_y(2, 0).start()
    row_y(2, 1).start()

    g_local(0, 2)
    for c in range(2):
        for lead in range(3):
            g_near(lead, c)
    g_local(2, n)
    g_side(0)
    for lead in range(3):
        g_far(lead, 0)
    g_near(2, 2)
    g_side(1)
    g_far(2, 1)
    g_far(0, 1)
    g_near(2, 3)
    g_near(2, 4)
    g_slot(0, 0)
    g_near(0, 2)
    g_far(1, 1)
    rows_hop1(0, 0)
    g_side(2)
    g_far(2, 2)
    g_near(2, 5)
    g_near(2, 6)
    for s in middle:
        g_slot(0, s)
    g_slot(1, 0)
    g_far(0, 2)
    rows_hop1(0, 1)
    g_own(1, 2)
    g_side(3)
    g_far(2, 3)
    over(7, n, lambda c: g_near(2, c))
    rows_hop2(0)
    g_own(1, 3)
    rows_hop1(1, 0)
    rows_ready(0)
    transpose(rows_s, s_t)
    g_slot(0, L - 2)
    for s in middle:
        g_slot(1, s)
    g_near(0, 3)
    rows_hop1(1, 1)
    g_side(4)
    g_far(2, 4)
    g_own(1, 4)
    rows_hop2(1)
    g_slot(1, L - 2)
    g_side(5)
    g_far(2, 5)
    rows_ready(1)
    transpose(rows_u, u_t)
    g_lead(2)
    g_slot_ahead(2, 0)
    g_far(0, 3)
    g_own(1, 5)
    over(6, n - 1, g_side)
    over(6, n - 1, lambda c: g_far(2, c))
    saved_part(0)
    g_side(n - 1)
    g_far(2, n - 1)
    g_own(1, 6)
    for s in middle:
        g_slot_ahead(2, s)
    saved_part(1)
    g_slot_ahead(2, L - 2)
    rows_hop1(2, 0)
    rows_hop1(2, 1)
    g_slot_ahead(3, 0)
    g_own(0, 4)
    over(7, n, lambda c: g_own(1, c))
    for s in middle:
        g_slot_ahead(3, s)
    s_last(2, 0)
    saved_part(2)
    mid_slots(0)
    g_slot_ahead(3, L - 2)

    def fresh_start():
        rows_hop2(2)
        rows_ready(2)
        over(0, 3, fresh_part)
        mid_slots(1)

    def period(c):
        g_slot_ahead(c, 0)
        pl.when(c + 1 < n)(lambda: g_own(0, c + 1))
        for s in middle:
            g_slot_ahead(c, s)
        pl.when(c == 4)(fresh_start)
        saved_part(c - 1)
        fresh_part(c - 1)
        mid_slots(c - 2)
        pl.when(c < n - 1)(lambda: s_last(2, c - 3))
        pl.when(c >= 5)(lambda: s_last(1, c - 5))
        g_slot_ahead(c, L - 2)

    over(4, n, period)

    def at_ends(c):
        pl.when(at_end)(lambda: finish(c))

    def inside(c):
        pl.when(jnp.logical_not(at_end))(lambda: finish(c))

    over(0, n - 3, lambda c: s_last(0, c))
    s_last(1, n - 5)
    s_last(1, n - 4)
    fresh_part(n - 1)
    for a in (0, 2):
        rows_sent(a)
    out_c(0, 0)
    out_c(0, 1)
    out_x(0, 0)
    out_x(0, 1)
    at_ends(0)

    def fresh_rest():
        out_c(0, 2)
        out_c(0, 3)
        out_x(0, 2)
        out_x(0, 3)

    pl.when(jnp.logical_not(at_end))(fresh_rest)
    inside(0)
    inside(1)
    mid_slots(n - 2)
    s_last(0, n - 3)
    s_last(1, n - 3)
    saved_part(n - 1)
    over(n - 4, n, lambda c: s_last(2, c))
    at_ends(1)
    inside(2)
    out_y(0, 0)
    pl.when(at_end)(fresh_rest)
    out_y(0, 1)
    at_ends(2)
    out_c(1, 0)
    out_c(1, 1)
    out_x(1, 0)
    mid_slots(n - 1)
    s_last(0, n - 2)
    s_last(1, n - 2)
    out_x(1, 1)
    finish(3)
    out_y(0, 2)
    out_c(1, 2)
    out_c(1, 3)
    out_x(1, 2)
    out_x(1, 3)
    s_last(1, n - 1)
    out_y(0, 3)
    over(4, n - 3, finish)
    s_last(0, n - 1)
    out_y(1, 0)
    finish(n - 3)
    out_y(1, 1)
    at_ends(n - 2)
    out_y(1, 2)
    inside(n - 2)
    at_ends(n - 1)
    out_y(1, 3)
    inside(n - 1)
    for h in range(PIECES):
        out_end(0, h)
    for h in range(PIECES):
        out_end(1, h)

    all_sent(w.at[:, :, 0:dp, :], sem_wys)
    for k in range(L):
        pl.when((z == k) & not_top)(lambda: all_sent(w.at[:, :, 0:(k + 1) * bd, :], sem_gs.at[0]))
        pl.when((z == k) & not_bottom)(lambda: all_sent(w.at[:, :, 0:(L - k) * bd, :], sem_gs.at[1]))
    all_sent(g.at[:, :, 0:(L - 1) * bd, :], sem_ss)
    for sem in (sem_fy, sem_fyr, sem_fl):
        all_sent(g.at[:, :, 0:dp, :], sem)
    all_sent(rows_s.at[0:3 * q, :], sem_rys)
    rows_sent(1)
    for a in range(2):
        for k, count in enumerate((half_rows, quarter, q)):
            all_sent(stages[a].at[0:count, :], sem_os.at[a, k])
        all_sent(stages[a].at[0:q, :], sem_ol.at[a])


def finish_kernel(grad_scale, fresh_in, saved_in, up_in, down_in, up_sum, down_sum, fresh, saved, up, down):
    fresh[...] = fresh_in[...]
    saved[...] = saved_in[...]
    up[...] = up_in[...] + grad_scale * up_sum[...].astype(F32)
    down[...] = down_in[...] + grad_scale * down_sum[...].astype(F32)


def finish_call(grad_scale, *arrays):
    steps = 2

    def spec(a):
        return pl.BlockSpec((a.shape[0] // steps, a.shape[1]), lambda i: (i, 0))

    outs = arrays[:4]
    return pl.pallas_call(
        functools.partial(finish_kernel, grad_scale),
        grid=(steps,),
        in_specs=[spec(a) for a in arrays],
        out_specs=[spec(a) for a in outs],
        out_shape=[jax.ShapeDtypeStruct(a.shape, a.dtype) for a in outs],
        cost_estimate=pl.CostEstimate(flops=2**20, bytes_accessed=2**24, transcendentals=0),
    )(*arrays)


def fused_body(plan, fresh_rows, saved_rows, upstream_grad, proj_up, proj_down, accum_up, accum_down):
    L, q, dp, K, H, n, cw, Tk = (plan[k] for k in ("L", "q", "dp", "K", "H", "n", "w", "Tk"))
    fs_n = lax.axis_size("fs")
    grad_scale = float(fresh_rows.shape[0] * fs_n) ** (-0.5)
    dma = lambda *shape: pltpu.SemaphoreType.DMA(shape)
    one = pltpu.SemaphoreType.DMA
    vm = lambda *shape: pltpu.VMEM(shape, BF)
    flops = 2 * 6 * Tk * K * H
    any_spec = pl.BlockSpec(memory_space=pl.ANY)
    fresh_out, saved_grad, up_sum, down_sum = pl.pallas_call(
        functools.partial(layer_kernel, plan),
        out_shape=(
            jax.ShapeDtypeStruct((q, K), BF),
            jax.ShapeDtypeStruct((q, K), BF),
            jax.ShapeDtypeStruct((dp, 2 * H), BF),
            jax.ShapeDtypeStruct((dp, 2 * H), BF),
        ),
        in_specs=[any_spec] * 5,
        out_specs=(any_spec,) * 4,
        scratch_shapes=[
            vm(Tk, K), vm(Tk, K), vm(Tk, K), vm(K, Tk), vm(K, Tk),
            vm(n, 2, K, cw), vm(n, Tk, cw), vm(n, Tk, cw), vm(Tk, cw),
            vm(n, 2, K, cw), vm(n, L + 1, 2, 2 * dp, cw),
            vm(2, Tk // 2, K), vm(2, Tk // 4, K), vm(2, q, K),
            dma(2), one, dma(n), dma(2), dma(n, L), one, dma(n, L + 1), one, one, one,
            dma(3), one, dma(3, 2), dma(3), dma(3), dma(3), dma(2, 3), dma(2, 3, PIECES), dma(2),
        ],
        compiler_params=pltpu.CompilerParams(
            collective_id=0, has_side_effects=True, vmem_limit_bytes=67043328),
        cost_estimate=pl.CostEstimate(flops=flops, bytes_accessed=2**24, transcendentals=0),
    )(fresh_rows, saved_rows, upstream_grad, proj_up, proj_down)
    return finish_call(grad_scale, fresh_out, saved_grad, accum_up, accum_down, up_sum, down_sum)


def any_body(*args):
    plan = make_plan(
        lax.axis_size("fs"), lax.axis_size("tp"), args[0].shape[0], args[0].shape[1],
        args[3].shape[0], args[3].shape[1], CHUNKS)
    if plan is None:
        return body(*args)
    return fused_body(plan, *args)


def solution(mesh):
    in_specs = (P("fs", None),) * 3 + (P("fs", "tp"),) * 4
    out_specs = (P(("fs", "tp"), None),) * 2 + (P("fs", "tp"),) * 2
    return jax.shard_map(any_body, mesh=mesh, in_specs=in_specs, out_specs=out_specs, check_vma=False)
```

```python
import functools

import jax
import jax.numpy as jnp
from jax import lax
from jax.experimental import pallas as pl
from jax.experimental.pallas import tpu as pltpu
from jax.sharding import PartitionSpec as P


BF = jnp.bfloat16
F32 = jnp.float32


def against_rows(left, right):
    return lax.dot_general(left, right, (((1,), (1,)), ((), ())), preferred_element_type=F32)


def over_tokens(left, right):
    return lax.dot_general(left, right, (((0,), (0,)), ((), ())), preferred_element_type=F32)


def squared_relu(pre_values):
    active = jnp.maximum(pre_values, 0.0)
    return (active, (active * active).astype(BF))


def after(value, *earlier):
    return lax.optimization_barrier((value, earlier))[0]


def body(fresh_rows, saved_rows, upstream_grad, proj_up, proj_down, accum_up, accum_down):
    fs_n, tp_n = lax.axis_size("fs"), lax.axis_size("tp")
    line_n = fs_n // 2
    fs, tp = lax.axis_index("fs"), lax.axis_index("tp")
    line, side = fs // 2, fs % 2
    row_count, width = fresh_rows.shape
    depth, columns = proj_up.shape
    half = columns // 2
    grad_scale = float(row_count * fs_n) ** (-0.5)

    def to_side(value):
        return lax.ppermute(value, "fs", [(i, i ^ 1) for i in range(fs_n)])

    def to_tp(value, bit):
        return lax.ppermute(value, "tp", [(j, j ^ bit) for j in range(tp_n)])

    def along(value, lines, way):
        return lax.ppermute(
            value,
            "fs",
            [(l * 2 + s, (l + way) * 2 + s) for l in lines for s in range(2)],
        )

    def side_block(weight):
        mine = lax.dynamic_slice_in_dim(weight, side * half, half, 1)
        other = lax.dynamic_slice_in_dim(weight, (1 - side) * half, half, 1)
        return mine, to_side(other)

    def line_gather(block, ties={}):
        ups, downs = [block], [block]
        for step in range(1, line_n):
            up, down = after((ups[-1], downs[-1]), *ties.get(step, ()))
            up = along(up, range(step - 1, line_n - 1), 1)
            down = along(down, range(1, line_n - step + 1), -1)
            up, down = lax.optimization_barrier((up, down))
            ups.append(up)
            downs.append(down)
        blocks = [block] + [
            jnp.where(line >= k, ups[k], downs[line_n - k]) for k in range(1, line_n)
        ]
        return jnp.concatenate(blocks, axis=0), ups

    def line_sum(grads, ties={}):
        size = 2 * depth
        up = down = None
        marks = []
        for step in range(1, line_n):
            low = grads[step * size : (step + 1) * size]
            high = grads[(line_n - step) * size : (line_n - step + 1) * size]
            low = low if up is None else low + up.astype(F32)
            high = high if down is None else high + down.astype(F32)
            low, high = after((low.astype(BF), high.astype(BF)), *ties.get(step, ()))
            up = along(low, range(0, step), 1)
            down = along(high, range(line_n - step, line_n), -1)
            up, down = lax.optimization_barrier((up, down))
            marks.append(up)
        return grads[:size] + up.astype(F32) + down.astype(F32), marks

    def finish_grad(accum, total, other):
        mine = total[:depth]
        other = other.astype(F32)
        return accum + jnp.where(
            side == 0,
            jnp.concatenate((mine, other), axis=1),
            jnp.concatenate((other, mine), axis=1),
        )

    order = [lax.rem(line - k + line_n, line_n) * 2 + (side ^ j) for k in range(line_n) for j in range(2)]
    core = tp % 2

    def near_rows(rows):
        piece = row_count // 2
        return to_side(lax.dynamic_slice_in_dim(rows, core * piece, piece, 0))

    def both_sides(rows, near):
        far = to_tp(near, 1)
        rows = jnp.concatenate(
            (rows, jnp.where(core == 0, near, far), jnp.where(core == 0, far, near)), axis=0
        )
        return jnp.concatenate(
            [lax.dynamic_slice_in_dim(rows, o * depth, depth, 1) for o in order], axis=1
        )

    def share_tp(term):
        value = term.astype(BF)
        bit, stages = 1, []
        outer = 2 * tp_n
        rest = row_count // tp_n
        value = value.reshape(2 * tp_n, rest, width)
        while bit < tp_n:
            outer //= 2
            view = value.reshape(outer, 2, rest, width)
            mine = (tp // bit) % 2
            keep = lax.dynamic_index_in_dim(view, mine, 1, keepdims=False)
            send = lax.dynamic_index_in_dim(view, 1 - mine, 1, keepdims=False)
            value = (keep.astype(F32) + to_tp(send, bit).astype(F32)).astype(BF)
            bit *= 2
            stages.append(value)
        return stages

    def share_side(value):
        blocks = [
            lax.dynamic_slice_in_dim(
                value, (lax.rem(line - b // 2 + line_n, line_n) * 2 + (side ^ (b % 2))) * depth, depth, 2
            )
            for b in range(fs_n)
        ]
        value = jnp.concatenate(blocks, axis=2)
        return (value[0].astype(F32) + to_side(value[1]).astype(F32)).astype(BF)

    up_pair = side_block(proj_up)
    down_pair = side_block(proj_down)
    rows = after((saved_rows, upstream_grad, fresh_rows), down_pair[1])
    nears = [near_rows(r) for r in rows]
    up_whole, ups = line_gather(jnp.concatenate(up_pair, axis=0))
    saved_all = both_sides(rows[0], after(nears[0], ups[max(line_n - 2, 1)]))
    upstream_all = both_sides(rows[1], after(nears[1], ups[-1]))
    down_start = after(jnp.concatenate(down_pair, axis=0), ups[-1])
    saved_pre = jnp.dot(saved_all, up_whole, preferred_element_type=F32)
    saved_active, saved_hidden = squared_relu(saved_pre)
    down_grads = grad_scale * over_tokens(upstream_all, saved_hidden)
    down_total, _ = line_sum(down_grads)
    fresh_all = both_sides(rows[2], after(nears[2], down_grads))
    fresh_hidden = squared_relu(jnp.dot(fresh_all, up_whole, preferred_element_type=F32))[1]
    down_whole, _ = line_gather(down_start, {2: (down_grads,), 3: (fresh_hidden,)})
    hidden_grad = jnp.dot(upstream_all, down_whole, preferred_element_type=F32)
    pre_grad = (2.0 * saved_active * hidden_grad).astype(BF)
    up_grads = grad_scale * over_tokens(saved_all, pre_grad)
    fresh_hidden, pre_grad, _ = lax.optimization_barrier((fresh_hidden, pre_grad, up_grads))
    fresh_stages = share_tp(against_rows(fresh_hidden, down_whole))
    saved_stages = share_tp(against_rows(pre_grad, up_whole))
    up_total, marks = line_sum(
        up_grads, {2: (fresh_stages[0], saved_stages[0]), 3: (fresh_stages[-1],)}
    )
    middle = marks[max(line_n - 3, 0)]
    fresh_out = share_side(fresh_stages[-1])
    saved_grad = share_side(saved_stages[-1])
    down_other = after(to_side(down_total[depth:].astype(BF)), middle)
    accum_down_out = finish_grad(accum_down, down_total, down_other)
    accum_up_out = finish_grad(accum_up, up_total, to_side(up_total[depth:].astype(BF)))
    return (fresh_out, saved_grad, accum_up_out, accum_down_out)


MESH = pl.DeviceIdType.MESH
CHUNKS = 8
ROW_TILE = 512
COL_TILE = 256
PIECES = 4


def make_plan(fs_n, tp_n, row_count, width, depth, columns, chunks):
    half = columns // 2
    if tp_n != 4 or fs_n % 2 or fs_n < 6 or half % chunks or (half // chunks) % 128 or chunks < 8 or chunks % 2 or fs_n < 8:
        return None
    if row_count % 128 or depth % 16 or width % (COL_TILE * PIECES):
        return None
    lines, tokens = fs_n // 2, 2 * row_count
    words = 5 * tokens * width + 2 * 2 * width * half + 2 * tokens * half + tokens * half // chunks
    words += 2 * (lines + 1) * 2 * depth * half + 2 * (tokens // 2 + tokens // 4 + tokens // 8) * width
    words += 2 * (tokens // 8) * width
    if 2 * words > 60 * 2**20:
        return None
    return dict(L=lines, q=row_count // 4, dp=depth, K=width, H=half, n=chunks, w=half // chunks, Tk=tokens)


def layer_kernel(plan, fresh_h, saved_h, upst_h, wu_h, wd_h, fo, so, gup, gdown,
                 rows_s, rows_u, rows_f, s_t, u_t, w, hid, pre, shid, g, gin, r1, r2, r3,
                 sem_wl, sem_wys, sem_wyr, sem_gs, sem_gr, sem_ss, sem_sr, sem_fy, sem_fyr, sem_fl,
                 sem_rl, sem_rys, sem_ryr, sem_rs, sem_rxr, sem_rdr, sem_os, sem_or, sem_ol):
    L, q, dp, K, H, n, cw, Tk = (plan[k] for k in ("L", "q", "dp", "K", "H", "n", "w", "Tk"))
    bd = 2 * dp
    gouts = (gup, gdown)
    fs, tp = lax.axis_index("fs"), lax.axis_index("tp")
    z, y = fs // 2, fs % 2
    x, c0 = tp // 2, tp % 2
    not_top, not_bottom = z < L - 1, z > 0
    dev_up, dev_down = (fs + 2, tp), (fs - 2, tp)
    dev_y = (z * 2 + (1 - y), tp)
    dev_x = (fs, (1 - x) * 2 + c0)
    dev_c = (fs, x * 2 + (1 - c0))

    def remote(src, dst, send, recv, dev):
        return pltpu.make_async_remote_copy(
            src_ref=src, dst_ref=dst, send_sem=send, recv_sem=recv, device_id=dev, device_id_type=MESH)

    def all_sent(ref, sem):
        pltpu.make_async_copy(ref, ref, sem).wait()

    def al(value, size):
        return pl.multiple_of(value, size)

    barrier = pltpu.get_barrier_semaphore()

    def greet(dev):
        pl.semaphore_signal(barrier, inc=1, device_id=dev, device_id_type=MESH)

    def w_cols(c, side):
        return pl.ds(al(side * H + c * cw, 128), cw)

    w_src = (wu_h, wd_h)
    my_rows = pl.ds(al((z * 2 + y) * dp, dp), dp)
    side_rows = pl.ds(al((z * 2 + 1 - y) * dp, dp), dp)

    def w_local(c, p):
        return pltpu.make_async_copy(
            w_src[p].at[:, w_cols(c, y)], w.at[c, p, my_rows, :], sem_wl.at[jnp.where(c < 2, 0, 1)])

    def w_side(c, p):
        return remote(
            w_src[p].at[:, w_cols(c, 1 - y)], w.at[c, p, my_rows, :], sem_wys, sem_wyr.at[c], dev_y)

    def start_w(c):
        for p in range(2):
            w_side(c, p).start()

    def w_start_local(c):
        for p in range(2):
            w_local(c, p).start()

    def g_copy(c, b, way):
        part = w.at[c, :, pl.ds(al(b * bd, bd), bd), :]
        return remote(part, part, sem_gs.at[way], sem_gr.at[c, b], (dev_up, dev_down)[way])

    def g_local(low, high):
        all_sent(w.at[low:high, :, my_rows, :], sem_wl.at[0 if low == 0 else 1])

    def g_side(c):
        all_sent(w.at[c, :, side_rows, :], sem_wyr.at[c])

    def by_lead(lead, up, down):
        leads = range(lead, L - 1) if lead == 2 else (lead,)
        for a in leads:
            pl.when(z == L - 2 - a)(up)
            pl.when(z == 1 + a)(down)

    def g_part(c, side, way):
        rows = w.at[c, :, pl.ds(al((z * 2 + side) * dp, dp), dp), :]
        remote(rows, rows, sem_gs.at[way], sem_gr.at[c, z], (dev_up, dev_down)[way]).start()

    def g_near(lead, c):
        by_lead(lead, lambda: g_part(c, y, 0), lambda: g_part(c, y, 1))

    def g_far(lead, c):
        by_lead(lead, lambda: g_part(c, 1 - y, 0), lambda: g_part(c, 1 - y, 1))

    def g_own(lead, c):
        g_near(lead, c)
        g_far(lead, c)

    def s_last(lead, c):
        by_lead(lead, lambda: s_slot_up(c, L - 2), lambda: s_slot_down(c, L - 2))

    at_end = (z == 0) | (z == L - 1)

    def g_low(c, s):
        low = z - 1 - s

        @pl.when(low >= 0)
        def _():
            g_copy(c, low, 0).wait_recv()
            pl.when(not_top)(lambda: g_copy(c, low, 0).start())

    def g_high(c, s):
        high = z + 1 + s

        @pl.when(high <= L - 1)
        def _():
            g_copy(c, high, 1).wait_recv()
            pl.when(not_bottom)(lambda: g_copy(c, high, 1).start())

    def g_slot(c, s):
        g_low(c, s)
        g_high(c, s)

    def g_lead(c):
        for ahead in range(1, L - 2):
            for k in range(ahead):
                for s in range(L - 2 - ahead):
                    pl.when(z == L - 2 - ahead)(lambda: g_low(c + k, s))
                    pl.when(z == 1 + ahead)(lambda: g_high(c + k, s))

    def g_slot_ahead(c, s):
        for ahead in range(L - 2):
            fits = c + ahead < n
            pl.when((z == L - 2 - ahead) & fits)(lambda: g_low(c + ahead, s))
            pl.when((z == 1 + ahead) & fits)(lambda: g_high(c + ahead, s))
        pl.when(z == L - 1)(lambda: g_low(c, s))
        pl.when(z == 0)(lambda: g_high(c, s))

    def block(c, b):
        return g.at[c, :, pl.ds(al(b * bd, bd), bd), :]

    def s_up(c, b):
        return remote(block(c, b), gin.at[c, b], sem_ss, sem_sr.at[c, b], dev_up)

    def s_down(c, b):
        return remote(block(c, b), gin.at[c, b], sem_ss, sem_sr.at[c, b], dev_down)

    def s_last_down(c, b):
        return remote(block(c, b), gin.at[c, L], sem_ss, sem_sr.at[c, L], dev_down)

    def add_in(c, b, *slots):
        for p in range(2):
            rows = pl.ds(al(b * bd, bd), bd)
            value = g[c, p, rows, :].astype(F32)
            for slot in slots:
                value = value + gin[c, slot, p].astype(F32)
            g[c, p, rows, :] = value.astype(BF)

    def s_slot_up(c, s):
        @pl.when((z <= s) & not_top)
        def _():
            b = L - 1 - s + z

            @pl.when(not_bottom)
            def _():
                s_up(c, b).wait_recv()
                add_in(c, b, b)

            s_up(c, b).start()

    def s_slot_down(c, s):
        @pl.when((L - 1 - z <= s) & not_bottom)
        def _():
            b = s - (L - 1) + z

            @pl.when(not_top)
            def _():
                s_down(c, b).wait_recv()
                add_in(c, b, b)

            if s == L - 2:
                s_last_down(c, b).start()
            else:
                s_down(c, b).start()

    def s_slot(c, s):
        s_slot_up(c, s)
        s_slot_down(c, s)

    def fin_side(c, p):
        return remote(
            g.at[c, p, pl.ds(al((z * 2 + 1 - y) * dp, dp), dp), :], gouts[p].at[:, w_cols(c, y)],
            sem_fy, sem_fyr, dev_y)

    def fin_local(c, p):
        return pltpu.make_async_copy(
            g.at[c, p, pl.ds(al((z * 2 + y) * dp, dp), dp), :], gouts[p].at[:, w_cols(c, y)], sem_fl)

    def finish(c):
        pl.when(not_bottom)(lambda: s_up(c, z).wait_recv())
        pl.when(not_top)(lambda: s_last_down(c, z).wait_recv())
        pl.when(z == 0)(lambda: add_in(c, z, L))
        pl.when(z == L - 1)(lambda: add_in(c, z, L - 1))
        pl.when(not_top & not_bottom)(lambda: add_in(c, z, z, L))
        for p in range(2):
            fin_side(c, p).start()
            fin_local(c, p).start()

    row_src = (saved_h, upst_h, fresh_h)
    row_dst = (rows_s, rows_u, rows_f)

    def spot(cc, xx, yy):
        return pl.ds(al(((cc * 2 + xx) * 2 + yy) * q, q), q)

    def row_local(a, j):
        return pltpu.make_async_copy(
            row_src[a].at[pl.ds(j * q, q), :], row_dst[a].at[spot(j % 2, j // 2, y), :], sem_rl.at[a])

    half_q = q // 2

    def spot_piece(cc, xx, yy, k):
        return pl.ds(al(((cc * 2 + xx) * 2 + yy) * q + k * half_q, half_q), half_q)

    def row_y(a, k):
        return remote(
            row_src[a].at[pl.ds(al(tp * q + k * half_q, half_q), half_q), :],
            row_dst[a].at[spot_piece(c0, x, y, k), :], sem_rys, sem_ryr.at[a, k], dev_y)

    def row_start(a):
        for k in range(2):
            row_y(a, k).start()

    def x_fwd(a, k):
        part = row_dst[a].at[spot_piece(c0, x, 1 - y, k), :]
        return remote(part, part, sem_rs.at[a], sem_rxr.at[a], dev_x)

    def d_fwd(a, k):
        part = row_dst[a].at[spot(c0, x if k == 0 else 1 - x, 1 - y), :]
        return remote(part, part, sem_rs.at[a], sem_rdr.at[a], dev_c)

    def rows_hop1(a, k):
        row_y(a, k).wait_recv()
        x_fwd(a, k).start()
        if k == 1:
            d_fwd(a, 0).start()

    def rows_hop2(a):
        all_sent(row_dst[a].at[spot(c0, 1 - x, 1 - y), :], sem_rxr.at[a])
        d_fwd(a, 1).start()

    def rows_sent(a):
        all_sent(row_dst[a].at[0:3 * q, :], sem_rs.at[a])

    def rows_ready(a):
        all_sent(row_dst[a].at[0:4 * q, :], sem_rl.at[a])
        all_sent(row_dst[a].at[0:2 * q, :], sem_rdr.at[a])

    def transpose(src, dst):
        tile = COL_TILE

        def step(i, carry):
            at = pl.ds(al(i * tile, tile), tile)
            dst[at, :] = src[:, at].T
            return carry

        lax.fori_loop(0, K // tile, step, 0)

    tm = min(ROW_TILE, Tk)

    def dot(a, b):
        return jnp.dot(a, b, preferred_element_type=F32)

    def saved_part(c):
        def step(t, carry):
            r = pl.ds(al(t * tm, tm), tm)
            active = jnp.maximum(dot(rows_s[r, :], w[c, 0]), 0.0)
            shid[r, :] = (active * active).astype(BF)
            pre[c, r, :] = (2.0 * active * dot(rows_u[r, :], w[c, 1])).astype(BF)
            return carry

        lax.fori_loop(0, Tk // tm, step, 0)

        def grad(i, carry):
            b = jnp.where(2 * z < L, L - 1 - i, i)
            r = pl.ds(al(b * bd, bd), bd)
            g[c, 0, r, :] = dot(s_t[r, :], pre[c]).astype(BF)
            g[c, 1, r, :] = dot(u_t[r, :], shid[...]).astype(BF)
            return carry

        lax.fori_loop(0, 1, grad, 0)
        s_slot(c, 0)
        lax.fori_loop(1, L, grad, 0)
        pl.when(at_end)(lambda: end_slots(c))

    def fresh_part(c):
        def step(t, carry):
            r = pl.ds(al(t * tm, tm), tm)
            active = jnp.maximum(dot(rows_f[r, :], w[c, 0]), 0.0)
            hid[c, r, :] = (active * active).astype(BF)
            return carry

        lax.fori_loop(0, Tk // tm, step, 0)

    half_rows = Tk // 2

    pw = K // PIECES

    def out_piece(a, cc, h):
        left, stage, p = ((hid, rows_f, 1), (pre, rows_s, 0))[a]
        r = pl.ds(al(cc * half_rows, half_rows), half_rows)

        def step(d, carry):
            at = pl.ds(al(h * pw + d * COL_TILE, COL_TILE), COL_TILE)
            total = None
            for c in range(0, n, 2):
                term = against_rows(
                    jnp.concatenate((left[c, r, :], left[c + 1, r, :]), axis=1),
                    jnp.concatenate((w[c, p, at, :], w[c + 1, p, at, :]), axis=1))
                total = term if total is None else total + term
            stage[r, at] = total.astype(BF)
            return carry

        lax.fori_loop(0, pw // COL_TILE, step, 0)

    stages = (rows_f, rows_s)
    quarter = Tk // 4
    far_x = pl.ds(al(c0 * half_rows + (1 - x) * quarter, quarter), quarter)

    def cols(h):
        return pl.ds(h * pw, pw)

    def o1(a, h):
        return remote(
            stages[a].at[pl.ds(al((1 - c0) * half_rows, half_rows), half_rows), cols(h)], r1.at[a, :, cols(h)],
            sem_os.at[a, 0], sem_or.at[a, 0, h], dev_c)

    def o2(a, h):
        return remote(
            stages[a].at[far_x, cols(h)], r2.at[a, :, cols(h)], sem_os.at[a, 1], sem_or.at[a, 1, h], dev_x)

    def o3(a, h):
        return remote(
            stages[a].at[spot(c0, x, 1 - y), cols(h)], r3.at[a, :, cols(h)],
            sem_os.at[a, 2], sem_or.at[a, 2, h], dev_y)

    def join(a, at, h, *terms):
        value = stages[a][at, cols(h)].astype(F32)
        for t in terms:
            value = value + t.astype(F32)
        return value

    def out_c(a, h):
        out_piece(a, 1 - c0, h)
        o1(a, h).start()

    def out_x(a, h):
        out_piece(a, c0, h)
        out_join(a, h)

    def y_first(a, h):
        return a == 0 and h == 0

    def o2_side(a, h, k):
        return remote(
            stages[a].at[spot(c0, k, 1 - y), cols(h)], r2.at[a, pl.ds(k * q, q), cols(h)],
            sem_os.at[a, 1], sem_or.at[a, 1, h], dev_y)

    def o3_far(a, h):
        return remote(
            stages[a].at[spot(c0, 1 - x, y), cols(h)], r3.at[a, :, cols(h)],
            sem_os.at[a, 2], sem_or.at[a, 2, h], dev_x)

    def side_pieces(a, xx, h):
        return (r1[a, pl.ds(al(xx * quarter + y * q, q), q), cols(h)],
                r2[a, pl.ds(al(xx * q, q), q), cols(h)])

    def out_join(a, h):
        o1(a, h).wait_recv()
        if y_first(a, h):
            for k in range(2):
                at = spot(c0, k, 1 - y)
                part = r1[a, pl.ds(al(k * quarter + (1 - y) * q, q), q), cols(h)]
                stages[a][at, cols(h)] = join(a, at, h, part).astype(BF)
                o2_side(a, h, k).start()
            return
        part = r1[a, pl.ds(al((1 - x) * quarter, quarter), quarter), cols(h)]
        stages[a][far_x, cols(h)] = join(a, far_x, h, part).astype(BF)
        o2(a, h).start()

    def out_pair(a, h):
        out_c(a, h)
        out_c(a, h + 1)
        out_x(a, h)
        out_x(a, h + 1)

    def pieces(a, yy, h):
        return (r1[a, pl.ds(al(x * quarter + yy * q, q), q), cols(h)],
                r2[a, pl.ds(al(yy * q, q), q), cols(h)])

    def out_y(a, h):
        if y_first(a, h):
            all_sent(r2.at[a, :, cols(h)], sem_or.at[a, 1, h])
            at = spot(c0, 1 - x, y)
            stages[a][at, cols(h)] = join(a, at, h, *side_pieces(a, 1 - x, h)).astype(BF)
            o3_far(a, h).start()
            return
        o2(a, h).wait_recv()
        at = spot(c0, x, 1 - y)
        stages[a][at, cols(h)] = join(a, at, h, *pieces(a, 1 - y, h)).astype(BF)
        o3(a, h).start()

    def out_local(a, h):
        return pltpu.make_async_copy(
            stages[a].at[spot(c0, x, y), cols(h)], (fo, so)[a].at[:, cols(h)], sem_ol.at[a])

    def out_end(a, h):
        o3(a, h).wait_recv()
        at = spot(c0, x, y)
        parts = side_pieces(a, x, h) if y_first(a, h) else pieces(a, y, h)
        stages[a][at, cols(h)] = join(a, at, h, *parts, r3[a, :, cols(h)]).astype(BF)
        out_local(a, h).start()

    def end_slots(c):
        for s in range(1, L - 2):
            s_slot(c, s)

    def mid_slots(c):
        pl.when(jnp.logical_not(at_end))(lambda: end_slots(c))

    def over(low, high, fn):
        if high > low:
            lax.fori_loop(low, high, lambda c, carry: (fn(c), carry)[1], 0)

    middle = range(1, L - 2)
    for c in range(2):
        w_start_local(c)
    pl.when(not_top)(lambda: greet(dev_up))
    pl.when(not_bottom)(lambda: greet(dev_down))
    greet(dev_y)
    greet(dev_x)
    greet(dev_c)
    over(2, n, w_start_local)
    for a in range(3):
        for j in range(4):
            row_local(a, j).start()
    pl.semaphore_wait(barrier, 3 + jnp.where(not_top, 1, 0) + jnp.where(not_bottom, 1, 0))
    start_w(0)
    start_w(1)
    row_y(0, 0).start()
    start_w(2)
    row_y(0, 1).start()
    start_w(3)
    row_y(1, 0).start()
    row_y(1, 1).start()
    over(4, n, start_w)
    row_y(2, 0).start()
    row_y(2, 1).start()

    g_local(0, 2)
    for c in range(2):
        for lead in range(3):
            g_near(lead, c)
    g_local(2, n)
    g_side(0)
    for lead in range(3):
        g_far(lead, 0)
    g_near(2, 2)
    g_side(1)
    g_far(2, 1)
    g_far(0, 1)
    g_near(2, 3)
    g_near(2, 4)
    g_slot(0, 0)
    g_near(0, 2)
    g_far(1, 1)
    rows_hop1(0, 0)
    g_side(2)
    g_far(2, 2)
    g_near(2, 5)
    g_near(2, 6)
    for s in middle:
        g_slot(0, s)
    g_slot(1, 0)
    g_far(0, 2)
    rows_hop1(0, 1)
    g_own(1, 2)
    g_side(3)
    g_far(2, 3)
    over(7, n, lambda c: g_near(2, c))
    rows_hop2(0)
    g_own(1, 3)
    rows_hop1(1, 0)
    rows_ready(0)
    transpose(rows_s, s_t)
    g_slot(0, L - 2)
    for s in middle:
        g_slot(1, s)
    g_near(0, 3)
    rows_hop1(1, 1)
    g_side(4)
    g_far(2, 4)
    g_own(1, 4)
    rows_hop2(1)
    g_slot(1, L - 2)
    g_side(5)
    g_far(2, 5)
    rows_ready(1)
    transpose(rows_u, u_t)
    g_lead(2)
    g_slot_ahead(2, 0)
    g_far(0, 3)
    g_own(1, 5)
    over(6, n - 1, g_side)
    over(6, n - 1, lambda c: g_far(2, c))
    saved_part(0)
    g_side(n - 1)
    g_far(2, n - 1)
    g_own(1, 6)
    for s in middle:
        g_slot_ahead(2, s)
    saved_part(1)
    g_slot_ahead(2, L - 2)
    rows_hop1(2, 0)
    rows_hop1(2, 1)
    g_slot_ahead(3, 0)
    g_own(0, 4)
    over(7, n, lambda c: g_own(1, c))
    for s in middle:
        g_slot_ahead(3, s)
    s_last(2, 0)
    saved_part(2)
    mid_slots(0)
    g_slot_ahead(3, L - 2)

    def fresh_start():
        rows_hop2(2)
        rows_ready(2)
        over(0, 3, fresh_part)
        mid_slots(1)

    def period(c):
        g_slot_ahead(c, 0)
        pl.when(c + 1 < n)(lambda: g_own(0, c + 1))
        for s in middle:
            g_slot_ahead(c, s)
        pl.when(c == 4)(fresh_start)
        saved_part(c - 1)
        fresh_part(c - 1)
        mid_slots(c - 2)
        pl.when(c < n - 1)(lambda: s_last(2, c - 3))
        pl.when(c >= 5)(lambda: s_last(1, c - 5))
        g_slot_ahead(c, L - 2)

    over(4, n, period)

    def at_ends(c):
        pl.when(at_end)(lambda: finish(c))

    def inside(c):
        pl.when(jnp.logical_not(at_end))(lambda: finish(c))

    over(0, n - 3, lambda c: s_last(0, c))
    s_last(1, n - 5)
    s_last(1, n - 4)
    fresh_part(n - 1)
    for a in (0, 2):
        rows_sent(a)
    out_c(0, 0)
    out_piece(0, c0, 0)
    out_c(0, 1)
    out_join(0, 0)
    out_c(0, 2)
    out_x(0, 1)
    out_x(0, 2)
    at_ends(0)

    def fresh_rest():
        out_c(0, 3)
        out_x(0, 3)

    pl.when(jnp.logical_not(at_end))(fresh_rest)
    inside(0)
    inside(1)
    inside(2)
    mid_slots(n - 2)
    pl.when(jnp.logical_not(at_end))(lambda: out_y(0, 0))
    s_last(0, n - 3)
    s_last(1, n - 3)
    saved_part(n - 1)
    over(n - 4, n, lambda c: s_last(2, c))
    at_ends(1)
    pl.when(at_end)(lambda: out_y(0, 0))
    pl.when(at_end)(fresh_rest)
    out_y(0, 1)
    at_ends(2)
    out_c(1, 0)
    out_c(1, 1)
    out_x(1, 0)
    mid_slots(n - 1)
    s_last(0, n - 2)
    s_last(1, n - 2)
    out_x(1, 1)
    finish(3)
    out_y(0, 2)
    out_c(1, 2)
    out_c(1, 3)
    out_x(1, 2)
    out_x(1, 3)
    s_last(1, n - 1)
    out_y(0, 3)

    def by_place(first, then):
        pl.when(jnp.logical_not(at_end))(first)
        pl.when(at_end)(then)

    pl.when(jnp.logical_not(at_end))(lambda: out_y(1, 0))
    over(4, n - 3, finish)
    s_last(0, n - 1)
    by_place(lambda: out_y(1, 1), lambda: out_y(1, 0))
    finish(n - 3)
    out_end(0, 0)
    out_end(0, 1)
    pl.when(at_end)(lambda: out_y(1, 1))
    out_end(0, 2)
    at_ends(n - 2)
    out_end(0, 3)
    out_y(1, 2)
    inside(n - 2)
    at_ends(n - 1)
    out_end(1, 0)
    out_y(1, 3)
    inside(n - 1)
    for h in range(1, PIECES):
        out_end(1, h)

    all_sent(w.at[:, :, 0:dp, :], sem_wys)
    for k in range(L):
        pl.when((z == k) & not_top)(lambda: all_sent(w.at[:, :, 0:(k + 1) * bd, :], sem_gs.at[0]))
        pl.when((z == k) & not_bottom)(lambda: all_sent(w.at[:, :, 0:(L - k) * bd, :], sem_gs.at[1]))
    all_sent(g.at[:, :, 0:(L - 1) * bd, :], sem_ss)
    for sem in (sem_fy, sem_fyr, sem_fl):
        all_sent(g.at[:, :, 0:dp, :], sem)
    all_sent(rows_s.at[0:3 * q, :], sem_rys)
    rows_sent(1)
    for a in range(2):
        for k, count in enumerate((half_rows, quarter, q)):
            all_sent(stages[a].at[0:count, :], sem_os.at[a, k])
        all_sent(stages[a].at[0:q, :], sem_ol.at[a])


def finish_kernel(grad_scale, fresh_in, saved_in, up_in, down_in, up_sum, down_sum, fresh, saved, up, down):
    fresh[...] = fresh_in[...]
    saved[...] = saved_in[...]
    up[...] = up_in[...] + grad_scale * up_sum[...].astype(F32)
    down[...] = down_in[...] + grad_scale * down_sum[...].astype(F32)


def finish_call(grad_scale, *arrays):
    steps = 2

    def spec(a):
        return pl.BlockSpec((a.shape[0] // steps, a.shape[1]), lambda i: (i, 0))

    outs = arrays[:4]
    return pl.pallas_call(
        functools.partial(finish_kernel, grad_scale),
        grid=(steps,),
        in_specs=[spec(a) for a in arrays],
        out_specs=[spec(a) for a in outs],
        out_shape=[jax.ShapeDtypeStruct(a.shape, a.dtype) for a in outs],
        cost_estimate=pl.CostEstimate(flops=2**20, bytes_accessed=2**24, transcendentals=0),
    )(*arrays)


def fused_body(plan, fresh_rows, saved_rows, upstream_grad, proj_up, proj_down, accum_up, accum_down):
    L, q, dp, K, H, n, cw, Tk = (plan[k] for k in ("L", "q", "dp", "K", "H", "n", "w", "Tk"))
    fs_n = lax.axis_size("fs")
    grad_scale = float(fresh_rows.shape[0] * fs_n) ** (-0.5)
    dma = lambda *shape: pltpu.SemaphoreType.DMA(shape)
    one = pltpu.SemaphoreType.DMA
    vm = lambda *shape: pltpu.VMEM(shape, BF)
    flops = 2 * 6 * Tk * K * H
    any_spec = pl.BlockSpec(memory_space=pl.ANY)
    fresh_out, saved_grad, up_sum, down_sum = pl.pallas_call(
        functools.partial(layer_kernel, plan),
        out_shape=(
            jax.ShapeDtypeStruct((q, K), BF),
            jax.ShapeDtypeStruct((q, K), BF),
            jax.ShapeDtypeStruct((dp, 2 * H), BF),
            jax.ShapeDtypeStruct((dp, 2 * H), BF),
        ),
        in_specs=[any_spec] * 5,
        out_specs=(any_spec,) * 4,
        scratch_shapes=[
            vm(Tk, K), vm(Tk, K), vm(Tk, K), vm(K, Tk), vm(K, Tk),
            vm(n, 2, K, cw), vm(n, Tk, cw), vm(n, Tk, cw), vm(Tk, cw),
            vm(n, 2, K, cw), vm(n, L + 1, 2, 2 * dp, cw),
            vm(2, Tk // 2, K), vm(2, Tk // 4, K), vm(2, q, K),
            dma(2), one, dma(n), dma(2), dma(n, L), one, dma(n, L + 1), one, one, one,
            dma(3), one, dma(3, 2), dma(3), dma(3), dma(3), dma(2, 3), dma(2, 3, PIECES), dma(2),
        ],
        compiler_params=pltpu.CompilerParams(
            collective_id=0, has_side_effects=True, vmem_limit_bytes=67043328),
        cost_estimate=pl.CostEstimate(flops=flops, bytes_accessed=2**24, transcendentals=0),
    )(fresh_rows, saved_rows, upstream_grad, proj_up, proj_down)
    return finish_call(grad_scale, fresh_out, saved_grad, accum_up, accum_down, up_sum, down_sum)


def any_body(*args):
    plan = make_plan(
        lax.axis_size("fs"), lax.axis_size("tp"), args[0].shape[0], args[0].shape[1],
        args[3].shape[0], args[3].shape[1], CHUNKS)
    if plan is None:
        return body(*args)
    return fused_body(plan, *args)


def solution(mesh):
    in_specs = (P("fs", None),) * 3 + (P("fs", "tp"),) * 4
    out_specs = (P(("fs", "tp"), None),) * 2 + (P("fs", "tp"),) * 2
    return jax.shard_map(any_body, mesh=mesh, in_specs=in_specs, out_specs=out_specs, check_vma=False)
```
